32 devices in a mesh: ep: 8 (over z, x), tp: 4 (over y, core).
Axes of the slice: x: 2, y: 2, z: 4, core: 2. Of those that a mesh axis runs over, the one named last changes fastest.
Arguments:
- hidden_in: bfloat16 [128, 4096], P('ep'), may hold values from -6 to 6
- w_query: bfloat16 [4096, 2048], P('ep', 'tp'), may hold values from -0.09375 to 0.09375
- w_key: bfloat16 [4096, 2048], P('ep', 'tp'), may hold values from -0.09375 to 0.09375
- w_value: bfloat16 [4096, 2048], P('ep', 'tp'), may hold values from -0.09375 to 0.09375
- w_outgate: bfloat16 [4096, 2048], P('ep', 'tp'), may hold values from -0.09375 to 0.09375
- w_igate: bfloat16 [4096, 16], P('ep', 'tp'), may hold values from -0.09375 to 0.09375
- w_fgate: bfloat16 [4096, 16], P('ep', 'tp'), may hold values from -0.09375 to 0.09375
- input_bias: float32 [16], P('tp'), may hold values from -3 to 303
- forget_bias: float32 [16], P('tp'), may hold values from -1 to 5
- mem_state: float32 [128, 16, 16384], P('ep', 'tp'), may hold values from -4 to 4
- max_state: float32 [128, 16], P('ep', 'tp'), may hold values from -4 to 304
- head_gain: float32 [2048], P('tp'), may hold values from 0.1 to 1.9
- w_output: bfloat16 [2048, 4096], P('tp'), may hold values from -0.26367188 to 0.26367188
- first_gain: float32 [4096], replicated, may hold values from 0.35 to 3.25
- w_group_router: bfloat16 [4096, 2], replicated, may hold values from -0.09375 to 0.09375
- w_expert_router: bfloat16 [4096, 8], replicated, may hold values from -0.09375 to 0.09375
- expert_route: int32 [128, 2], P('ep'), may hold values from 0 to 7, as said below
- w_expgate: bfloat16 [8, 4096, 1024], P('ep', None, 'tp'), may hold values from -0.09375 to 0.09375
- w_expup: bfloat16 [8, 4096, 1024], P('ep', None, 'tp'), may hold values from -0.09375 to 0.09375
- w_expdown: bfloat16 [8, 1024, 4096], P('ep', 'tp'), may hold values from -0.75 to 0.75
- second_gain: float32 [4096], P('tp'), may hold values from 0.1 to 1.9
Outputs:
- hidden_out: bfloat16 [128, 4096], P('ep', 'tp')
- mem_next: float32 [128, 16, 16384], P('ep', 'tp')
- max_next: float32 [128, 16], P('ep', 'tp')
The draws below stay inside these ranges and needn't reach their ends.
Inputs may be any that keep to these rules, and one draw needn't show every extreme that they name: `expert_route`: each row names two different experts of one group (an expert's group is its number divided by 4). In each aligned block of 16 rows (the rows of one index of ep) every group is named by exactly 8 rows, no expert by more than 8 rows, and some expert by exactly 8 rows.
All inputs are finite; a program needn't handle non-finite values.
Results may differ from the reference program's by a relative error of at most 0.02.
Values may be sent and summed in bfloat16 or wider, within the bound.
A program may use at most 64 MiB of HBM per device.

```python
import jax
import jax.numpy as jnp
from jax import lax

D = 4096
HEADS = 16
DH = 128
HD = 2048
DE = 1024
GROUP_SIZE = 4
TOP_K = 2
EXPERTS = 8
GROUPS = 2
SEQ_DEV = 16
SEQUENCES = 128
CAP = 8
N_EP = 8
N_TP = 4


def draw_input_bias(key, part):
    base = jax.random.uniform(jax.random.fold_in(key, 1), (HEADS,), jnp.float32, -3.0, 3.0)
    return base


def draw_max_state(key, part):
    base = jax.random.uniform(jax.random.fold_in(key, 2), (SEQUENCES, HEADS), jnp.float32, -4.0, 4.0)
    return base


def draw_first_gain(key, part):
    positions = jnp.arange(D, dtype=jnp.float32) / D
    rough = jax.random.uniform(jax.random.fold_in(key, 3), (D,), jnp.float32, 0.7, 1.3)
    ramp = 0.5 * jnp.power(5.0, positions)
    return ramp * rough


def route_block(block_key):
    coin_key, forced_key, perm_key, swap_key, order_key = jax.random.split(block_key, 5)
    skewed = jax.random.randint(coin_key, (GROUPS,), 0, 2)
    forced = jax.random.randint(forced_key, (), 0, GROUPS)
    skewed = jnp.where(jnp.arange(GROUPS) == forced, 1, skewed)
    ranks_to_expert = jax.vmap(lambda one_key: jax.random.permutation(one_key, GROUP_SIZE))(jax.random.split(perm_key, GROUPS))
    skew_counts = jnp.array([CAP, 0, CAP // 2, CAP // 2], jnp.int32)
    even_counts = jnp.array([CAP // 2, CAP // 2, CAP // 2, CAP // 2], jnp.int32)
    counts = jnp.where(skewed[:, None] == 1, skew_counts[None, :], even_counts[None, :])
    running = jnp.cumsum(counts, 1)
    slots = jnp.arange(2 * CAP, dtype=jnp.int32)
    rank_of_slot = jnp.sum((slots[None, :, None] >= running[:, None, :]).astype(jnp.int32), -1)
    expert_of_slot = jnp.take_along_axis(ranks_to_expert, rank_of_slot, 1) + GROUP_SIZE * jnp.arange(GROUPS, dtype=jnp.int32)[:, None]
    pairs = jnp.stack([expert_of_slot[:, :CAP], expert_of_slot[:, CAP:]], -1).reshape(GROUPS * CAP, 2)
    swapped = jax.random.randint(swap_key, (GROUPS * CAP,), 0, 2)
    pairs = jnp.where(swapped[:, None] == 1, pairs[:, ::-1], pairs)
    order = jax.random.permutation(order_key, GROUPS * CAP)
    return pairs[order]


def draw_expert_route(key, part):
    block_keys = jax.random.split(jax.random.fold_in(key, 5), SEQUENCES // SEQ_DEV)
    routes = jax.vmap(route_block)(block_keys)
    return routes.reshape(SEQUENCES, TOP_K).astype(jnp.int32)


def shard_levels(rng, dims, cuts, least, largest):
    def one(position, parts):
        heights = jax.random.uniform(jax.random.fold_in(jax.random.fold_in(rng, 6), position), (parts,), jnp.float32, least / len(cuts), largest / len(cuts))
        return jnp.repeat(jnp.exp(heights), dims[position] // parts).reshape((-1,) + (1,) * (len(dims) - position - 1))

    level = one(*cuts[0])
    for cut in cuts[1:]:
        level = level * one(*cut)
    return level


def bell_draw(key, shape, deviation, reach, cuts=(), held_as=jnp.bfloat16):
    drawn = jax.random.normal(key, shape, jnp.float32) * deviation
    if len(cuts) > 0:
        drawn = shard_levels(key, shape, cuts, -0.22, 0.18) * drawn
    return jnp.clip(drawn, min=-reach, max=reach).astype(held_as)


def setup_inputs(seed: int = 0) -> dict:
    streams_of = jax.random.split(jax.random.key(seed), 22)
    return {
        "hidden_in": bell_draw(streams_of[0], (SEQUENCES, D), 1.0, 6.0, ((0, 8),)),
        "w_query": bell_draw(streams_of[1], (D, HD), D ** -0.5, 0.09375, ((0, 8), (1, 4))),
        "w_key": bell_draw(streams_of[2], (D, HD), D ** -0.5, 0.09375, ((0, 8), (1, 4))),
        "w_value": bell_draw(streams_of[3], (D, HD), D ** -0.5, 0.09375, ((0, 8), (1, 4))),
        "w_outgate": bell_draw(streams_of[4], (D, HD), D ** -0.5, 0.09375, ((0, 8), (1, 4))),
        "w_igate": bell_draw(streams_of[5], (D, HEADS), D ** -0.5, 0.09375, ((0, 8), (1, 4))),
        "w_fgate": bell_draw(streams_of[6], (D, HEADS), D ** -0.5, 0.09375, ((0, 8), (1, 4))),
        "input_bias": draw_input_bias(jax.random.fold_in(streams_of[21], 71), 0),
        "forget_bias": jnp.clip(-1.0 + 6.0 * jax.random.uniform(streams_of[8], (HEADS,), jnp.float32) ** shard_levels(streams_of[8], (HEADS,), ((0, 4),), -0.2, 0.2), -1.0, 5.0),
        "mem_state": bell_draw(streams_of[9], (SEQUENCES, HEADS, DH * DH), 0.5, 4.0, ((0, 8), (1, 4)), jnp.float32),
        "max_state": draw_max_state(jax.random.fold_in(streams_of[21], 71), 0),
        "head_gain": jnp.clip(1.0 + 0.18 * jax.random.normal(streams_of[11], (HD,), jnp.float32), 0.1, 1.9),
        "w_output": bell_draw(streams_of[12], (HD, D), (2.0 / HD ** 0.5), 0.26367188, ((0, 4),)),
        "first_gain": draw_first_gain(jax.random.fold_in(streams_of[21], 71), 0),
        "w_group_router": bell_draw(streams_of[14], (D, GROUPS), D ** -0.5, 0.09375),
        "w_expert_router": bell_draw(streams_of[15], (D, EXPERTS), D ** -0.5, 0.09375),
        "expert_route": draw_expert_route(jax.random.fold_in(streams_of[21], 71), 0),
        "w_expgate": bell_draw(streams_of[17], (EXPERTS, D, DE), D ** -0.5, 0.09375, ((0, 8), (2, 4))),
        "w_expup": bell_draw(streams_of[18], (EXPERTS, D, DE), D ** -0.5, 0.09375, ((0, 8), (2, 4))),
        "w_expdown": bell_draw(streams_of[19], (EXPERTS, DE, D), (4.0 / DE ** 0.5), 0.75, ((0, 8), (1, 4))),
        "second_gain": jnp.clip(1.0 + 0.18 * jax.random.normal(streams_of[20], (D,), jnp.float32), 0.1, 1.9),
    }


res_alpha = 8.0 ** 0.25

def layer_norm(values, gain):
    row_mean = lax.optimization_barrier(jnp.mean(values, -1, keepdims=True))
    row_var = lax.optimization_barrier(jnp.mean(values * values, -1, keepdims=True)) - row_mean * row_mean
    return (values - row_mean) * lax.rsqrt(row_var + 1e-05) * gain

def mlstm_step(queries, keys_scaled, values, log_input, log_forget, memory, stabilizer):
    new_max = jnp.maximum(log_forget + stabilizer, log_input)
    keep_old = jnp.exp(log_forget + stabilizer - new_max)
    write_new = jnp.exp(log_input - new_max)
    scores = lax.optimization_barrier(jnp.sum(queries * keys_scaled, -1)) * write_new
    read_old = jnp.einsum('bhd,bhde->bhe', queries, memory, precision=lax.Precision.HIGHEST)
    readout = scores[..., None] * values + keep_old[..., None] * read_old
    memory_next = keep_old[..., None, None] * memory + write_new[..., None, None] * keys_scaled[..., :, None] * values[..., None, :]
    return (readout, memory_next, new_max)

def head_mix(readout, head_gain, out_pre):
    scaled = readout * lax.rsqrt(lax.optimization_barrier(jnp.mean(readout * readout, -1, keepdims=True)) + 1e-06)
    flat_heads = scaled.reshape(scaled.shape[0], -1)
    return (flat_heads * head_gain * jax.nn.sigmoid(out_pre)).astype(jnp.bfloat16)

def route_weights(mid_float, w_group_router, w_expert_router, expert_route):
    group_logits = jnp.dot(mid_float, w_group_router.astype(jnp.float32), precision=lax.Precision.HIGHEST)
    expert_logits = jnp.dot(mid_float, w_expert_router.astype(jnp.float32), precision=lax.Precision.HIGHEST)
    first_expert = expert_route[:, 0]
    second_expert = expert_route[:, 1]
    expert_ids = lax.broadcasted_iota(jnp.int32, expert_logits.shape, 1)
    group_ids = lax.broadcasted_iota(jnp.int32, group_logits.shape, 1)
    first_logit = lax.optimization_barrier(jnp.sum(jnp.where(expert_ids == first_expert[:, None], expert_logits, 0.0), -1))
    second_logit = lax.optimization_barrier(jnp.sum(jnp.where(expert_ids == second_expert[:, None], expert_logits, 0.0), -1))
    group_pick = lax.optimization_barrier(jnp.sum(jnp.where(group_ids == (first_expert // GROUP_SIZE)[:, None], group_logits, 0.0), -1))
    group_gate = jax.nn.sigmoid(group_pick)
    return (group_gate * jax.nn.sigmoid(first_logit - second_logit), group_gate * jax.nn.sigmoid(second_logit - first_logit))

def slot_ranks(flat_routes, expert_total):
    onehot = (flat_routes[:, None] == lax.broadcasted_iota(jnp.int32, (flat_routes.shape[0], expert_total), 1)).astype(jnp.int32)
    running = jnp.cumsum(onehot, 0)
    return lax.optimization_barrier(jnp.sum((running - 1) * onehot, -1)).astype(jnp.int32)

def add_block(total, pieces):
    block_rows, block_weight = pieces
    partial_sum = jnp.dot(block_rows, block_weight, preferred_element_type=jnp.float32)
    partial_sum = lax.optimization_barrier(partial_sum.astype(jnp.bfloat16)).astype(jnp.float32)
    return (total + partial_sum, None)

def blocked_product(left, right):
    row_count = left.shape[0]
    inner = left.shape[1] // N_TP
    left_blocks = left.reshape(row_count, N_TP, inner).transpose(1, 0, 2)
    right_blocks = right.reshape(N_TP, inner, right.shape[1])
    total, unused = lax.scan(add_block, jnp.zeros((row_count, right.shape[1]), jnp.float32), (left_blocks, right_blocks))
    return total

def run_expert(pieces):
    rows_in, gate_weight, up_weight, down_weight = pieces
    gate_pre = jnp.dot(rows_in, gate_weight, preferred_element_type=jnp.float32)
    up_pre = jnp.dot(rows_in, up_weight, preferred_element_type=jnp.float32)
    hidden_units = (jax.nn.silu(gate_pre) * up_pre).astype(jnp.bfloat16)
    return blocked_product(hidden_units, down_weight).astype(jnp.bfloat16)

def reference(hidden_in, w_query, w_key, w_value, w_outgate, w_igate, w_fgate, input_bias, forget_bias, mem_state, max_state, head_gain, w_output, first_gain, w_group_router, w_expert_router, expert_route, w_expgate, w_expup, w_expdown, second_gain):
    shape4 = (SEQUENCES, HEADS, DH)
    queries = jnp.dot(hidden_in, w_query, preferred_element_type=jnp.float32).reshape(shape4)
    keys_scaled = jnp.dot(hidden_in, w_key, preferred_element_type=jnp.float32).reshape(shape4) * DH ** (-0.5)
    values = jnp.dot(hidden_in, w_value, preferred_element_type=jnp.float32).reshape(shape4)
    out_pre = jnp.dot(hidden_in, w_outgate, preferred_element_type=jnp.float32)
    log_input = jnp.dot(hidden_in, w_igate, preferred_element_type=jnp.float32) + input_bias
    log_forget = jax.nn.log_sigmoid(jnp.dot(hidden_in, w_fgate, preferred_element_type=jnp.float32) + forget_bias)
    memory = mem_state.reshape(SEQUENCES, HEADS, DH, DH)
    readout, mem_square, max_next = mlstm_step(queries, keys_scaled, values, log_input, log_forget, memory, max_state)
    mem_next = mem_square.reshape(SEQUENCES, HEADS, DH * DH)
    mixed_heads = head_mix(readout, head_gain, out_pre)
    mix = blocked_product(mixed_heads, w_output)
    mid_float = layer_norm(res_alpha * hidden_in.astype(jnp.float32) + mix, first_gain)
    mid = mid_float.astype(jnp.bfloat16)
    first_weight, second_weight = route_weights(mid_float, w_group_router, w_expert_router, expert_route)
    flat_routes = expert_route.reshape(-1).astype(jnp.int32)
    block_routes = flat_routes.reshape(N_EP, TOP_K * SEQ_DEV)
    ranks = jax.vmap(slot_ranks, in_axes=(0, None))(block_routes, EXPERTS).reshape(-1)
    source_block = (jnp.arange(SEQUENCES * TOP_K, dtype=jnp.int32) // (TOP_K * SEQ_DEV)).astype(jnp.int32)
    slot_index = ((flat_routes * N_EP + source_block) * CAP + ranks).astype(jnp.int32)
    repeated = jnp.repeat(mid, TOP_K, 0)
    buffer = jnp.zeros((EXPERTS * N_EP * CAP, D), jnp.bfloat16).at[slot_index].set(repeated)
    buffer = buffer.reshape(EXPERTS, N_EP * CAP, D)
    expert_out = lax.map(run_expert, (buffer, w_expgate, w_expup, w_expdown)).reshape(EXPERTS * N_EP * CAP, D)
    picked = expert_out[slot_index].astype(jnp.float32).reshape(SEQUENCES, TOP_K, D)
    moe = first_weight[:, None] * picked[:, 0] + second_weight[:, None] * picked[:, 1]
    joined = res_alpha * mid.astype(jnp.float32) + moe
    hidden_out = layer_norm(joined, second_gain).astype(jnp.bfloat16)
    return (hidden_out, mem_next, max_next)
```

```python
import functools

import jax
import jax.numpy as jnp
from jax import lax
from jax.experimental import pallas as pl
from jax.experimental.pallas import tpu as pltpu
from jax.sharding import PartitionSpec as P

D = 4096
DH = 128
GROUP_SIZE = 4
MESH = pl.DeviceIdType.MESH


res_alpha = 8.0**0.25


def layer_norm(values, gain):
    row_mean = jnp.mean(values, -1, keepdims=True)
    row_var = jnp.mean(values * values, -1, keepdims=True) - row_mean * row_mean
    return (values - row_mean) * lax.rsqrt(row_var + 1e-05) * gain


def mlstm_step(queries, keys_scaled, values, log_input, log_forget, memory, stabilizer):
    new_max = jnp.maximum(log_forget + stabilizer, log_input)
    keep_old = jnp.exp(log_forget + stabilizer - new_max)
    write_new = jnp.exp(log_input - new_max)
    scores = jnp.sum(queries * keys_scaled, -1) * write_new
    read_old = jnp.einsum("bhd,bhde->bhe", queries, memory, precision=lax.Precision.HIGHEST)
    readout = scores[..., None] * values + keep_old[..., None] * read_old
    memory_next = (
        keep_old[..., None, None] * memory
        + write_new[..., None, None] * keys_scaled[..., :, None] * values[..., None, :]
    )
    return (readout, memory_next, new_max)


def head_mix(readout, head_gain, out_pre):
    scaled = readout * lax.rsqrt(jnp.mean(readout * readout, -1, keepdims=True) + 1e-06)
    flat_heads = scaled.reshape(scaled.shape[0], -1)
    return (flat_heads * head_gain * jax.nn.sigmoid(out_pre)).astype(jnp.bfloat16)


def route_weights(mid_float, w_group_router, w_expert_router, expert_route):
    group_logits = jnp.dot(
        mid_float, w_group_router.astype(jnp.float32), precision=lax.Precision.HIGHEST
    )
    expert_logits = jnp.dot(
        mid_float, w_expert_router.astype(jnp.float32), precision=lax.Precision.HIGHEST
    )
    first_expert = expert_route[:, 0]
    second_expert = expert_route[:, 1]
    expert_ids = lax.broadcasted_iota(jnp.int32, expert_logits.shape, 1)
    group_ids = lax.broadcasted_iota(jnp.int32, group_logits.shape, 1)
    first_logit = jnp.sum(jnp.where(expert_ids == first_expert[:, None], expert_logits, 0.0), -1)
    second_logit = jnp.sum(jnp.where(expert_ids == second_expert[:, None], expert_logits, 0.0), -1)
    group_pick = jnp.sum(
        jnp.where(group_ids == (first_expert // GROUP_SIZE)[:, None], group_logits, 0.0), -1
    )
    group_gate = jax.nn.sigmoid(group_pick)
    return (
        group_gate * jax.nn.sigmoid(first_logit - second_logit),
        group_gate * jax.nn.sigmoid(second_logit - first_logit),
    )


def slot_ranks(flat_routes, expert_total):
    onehot = (
        flat_routes[:, None]
        == lax.broadcasted_iota(jnp.int32, (flat_routes.shape[0], expert_total), 1)
    ).astype(jnp.int32)
    running = jnp.cumsum(onehot, 0)
    return jnp.sum((running - 1) * onehot, -1)


def body(
    hidden_in,
    w_query,
    w_key,
    w_value,
    w_outgate,
    w_igate,
    w_fgate,
    input_bias,
    forget_bias,
    mem_state,
    max_state,
    head_gain,
    w_output,
    first_gain,
    w_group_router,
    w_expert_router,
    expert_route,
    w_expgate,
    w_expup,
    w_expdown,
    second_gain,
):
    own_rows, width = hidden_in.shape
    heads_here = mem_state.shape[1]
    head_width = heads_here * DH
    top_count = expert_route.shape[1]
    spread_rows = lax.all_to_all(hidden_in, "ep", split_axis=1, concat_axis=0, tiled=True)
    stacked_w = jnp.concatenate([w_query, w_key, w_value, w_outgate], 1)
    gate_w = jnp.concatenate([w_igate, w_fgate], 1)
    proj_terms = jnp.dot(spread_rows, stacked_w, preferred_element_type=jnp.float32)
    gate_terms = jnp.dot(spread_rows, gate_w, preferred_element_type=jnp.float32)
    projected, gate_sums = (
        lax.psum_scatter(proj_terms, "ep", scatter_dimension=0, tiled=True),
        lax.psum_scatter(gate_terms, "ep", scatter_dimension=0, tiled=True),
    )
    shaped = projected.reshape(own_rows, 4, heads_here, DH)
    queries = shaped[:, 0]
    keys_raw = shaped[:, 1]
    values = shaped[:, 2]
    out_pre = shaped[:, 3].reshape(own_rows, head_width)
    input_sum = gate_sums[:, :heads_here]
    forget_sum = gate_sums[:, heads_here:]
    keys_scaled = keys_raw * DH ** (-0.5)
    log_input = input_sum + input_bias
    log_forget = jax.nn.log_sigmoid(forget_sum + forget_bias)
    memory = mem_state.reshape(own_rows, heads_here, DH, DH)
    readout, memory_square, new_max = mlstm_step(
        queries, keys_scaled, values, log_input, log_forget, memory, max_state
    )
    memory_next = memory_square.reshape(own_rows, heads_here, DH * DH)
    mixed_heads = head_mix(readout, head_gain, out_pre)
    partial_mix = jnp.dot(mixed_heads, w_output, preferred_element_type=jnp.float32).astype(
        jnp.bfloat16
    )
    mix = lax.psum(partial_mix.astype(jnp.float32).astype(jnp.bfloat16), "tp").astype(jnp.float32)
    mid_float = layer_norm(res_alpha * hidden_in.astype(jnp.float32) + mix, first_gain)
    mid = mid_float.astype(jnp.bfloat16)
    first_weight, second_weight = route_weights(
        mid_float, w_group_router, w_expert_router, expert_route
    )
    expert_total = w_expgate.shape[0] * lax.axis_size("ep")
    capacity = 2 * own_rows * top_count // expert_total
    flat_routes = expert_route.reshape(-1)
    local_slot = flat_routes * capacity + slot_ranks(flat_routes, expert_total)
    share_width = width // lax.axis_size("tp")
    mid_share = lax.dynamic_slice_in_dim(mid, lax.axis_index("tp") * share_width, share_width, 1)
    buffer = (
        jnp.zeros((expert_total * capacity, width), jnp.bfloat16)
        .at[local_slot]
        .set(jnp.repeat(mid, top_count, 0))
    )
    arrived = lax.all_to_all(
        buffer.reshape(expert_total, capacity, width), "ep", split_axis=0, concat_axis=1, tiled=True
    )
    gate_pre = jnp.einsum("erd,edf->erf", arrived, w_expgate, preferred_element_type=jnp.float32)
    up_pre = jnp.einsum("erd,edf->erf", arrived, w_expup, preferred_element_type=jnp.float32)
    hidden_units = (jax.nn.silu(gate_pre) * up_pre).astype(jnp.bfloat16)
    down_terms = jnp.einsum(
        "erf,efd->erd", hidden_units, w_expdown, preferred_element_type=jnp.float32
    ).astype(jnp.bfloat16)
    expert_share = lax.psum_scatter(
        down_terms.astype(jnp.float32).astype(jnp.bfloat16), "tp", scatter_dimension=2, tiled=True
    )
    returned = lax.all_to_all(expert_share, "ep", split_axis=1, concat_axis=0, tiled=True)
    picked = returned.reshape(expert_total * capacity, share_width)[local_slot]
    picked = picked.astype(jnp.float32).reshape(own_rows, top_count, share_width)
    moe = first_weight[:, None] * picked[:, 0] + second_weight[:, None] * picked[:, 1]
    joined = res_alpha * mid_share.astype(jnp.float32) + moe
    row_sum, square_sum = lax.psum((jnp.sum(joined, -1), jnp.sum(joined * joined, -1)), "tp")
    row_mean = row_sum / D
    row_var = square_sum / D - row_mean * row_mean
    hidden_out = (
        (joined - row_mean[:, None]) * lax.rsqrt(row_var[:, None] + 1e-05) * second_gain
    ).astype(jnp.bfloat16)
    return (hidden_out, memory_next, new_max)


VMEM_LIMIT = 59 * 1024 * 1024


def announce(peers):
    barrier = pltpu.get_barrier_semaphore()
    for peer in peers:
        pl.semaphore_signal(barrier, inc=1, device_id=peer, device_id_type=MESH)
    return barrier


def remote(source, target, send_sem, recv_sem, peer):
    return pltpu.make_async_remote_copy(
        src_ref=source,
        dst_ref=target,
        send_sem=send_sem,
        recv_sem=recv_sem,
        device_id=peer,
        device_id_type=MESH,
    )


def flip(index, bits):
    result = index
    place = 1
    while place <= bits:
        if bits & place:
            result = result + place * (1 - 2 * lax.rem(lax.div(index, place), 2))
        place *= 2
    return result


def three_parts(value):
    high = value.astype(jnp.bfloat16).astype(jnp.float32)
    rest = value - high
    middle = rest.astype(jnp.bfloat16).astype(jnp.float32)
    return high, middle, rest - middle


def dot32(left, right):
    return jnp.dot(left, right, preferred_element_type=jnp.float32)


def dot_t(left, right):
    return lax.dot_general(left, right, (((1,), (1,)), ((), ())), preferred_element_type=jnp.float32)


def layer_kernel(
    n_ep,
    n_tp,
    groups,
    hidden_hbm,
    wq,
    wk,
    wv,
    wo,
    memory,
    w_out,
    w_gate,
    w_up,
    w_down,
    w_igate_t_hbm,
    w_fgate_t_hbm,
    input_bias_hbm,
    forget_bias_hbm,
    max_state_t_hbm,
    head_gain_hbm,
    gain1_hbm,
    gain2_hbm,
    group_router_t_hbm,
    expert_router_t_hbm,
    route_t_hbm,
    out_ref,
    mem_out,
    max_out,
    w_igate_t,
    w_fgate_t,
    input_bias,
    forget_bias,
    max_state_t,
    head_gain,
    gain1,
    gain2,
    group_router_t,
    expert_router_t,
    route_t,
    hid,
    weights,
    wo_buf,
    wg_buf,
    wu_buf,
    wd_buf,
    mem_half,
    gate_w,
    spread,
    proj_send,
    proj_recv,
    proj_own,
    far_own,
    far_recv,
    cross_send,
    cross_recv,
    cross_send2,
    cross_recv2,
    write_keys,
    keep_buf,
    value_buf,
    mix_send,
    mix_recv,
    sum_send,
    sum_recv,
    row_send,
    arrived,
    arrived2,
    stat_send,
    stat_recv,
    weight_buf,
    mid_buf,
    down_send,
    down_recv,
    ret_send,
    ret_recv,
    stat2_send,
    stat2_recv,
    load_sem,
    small_sem,
    h_send,
    h_recv,
    p_send,
    p_recv,
    f_send,
    f_recv,
    c_send,
    c_recv,
    m_send,
    m_recv,
    u_send,
    u_recv,
    a_send,
    a_recv,
    b_send,
    b_recv,
    s_send,
    s_recv,
    d_send,
    d_recv,
    r_send,
    r_recv,
    t_send,
    t_recv,
):
    me = lax.axis_index("ep")
    tp = lax.axis_index("tp")
    n_y = n_tp // 2
    y = lax.div(tp, 2)
    core = lax.rem(tp, 2)
    rows, width = hid.shape
    share = width // n_tp
    block = rows // groups
    heads = keep_buf.shape[0]
    depth, cols = wq.shape
    far_first = list(range(n_ep - 1, 0, -1))
    near_first = list(range(1, n_ep))
    ep_peer = [flip(me, k) for k in range(n_ep)]
    y_peer = [lax.rem(y + j, n_y) for j in range(n_y)]
    y_from = [lax.rem(y + n_y - j, n_y) for j in range(n_y)]
    tp_peer = [lax.rem(tp + o, n_tp) for o in range(n_tp)]
    partner = (me, 2 * y + 1 - core)
    started = []

    def begin(copy):
        copy.start()
        started.append(copy)
        return copy

    def share_of(index):
        return pl.ds(pl.multiple_of(index * share, share), share)

    peers = [(ep_peer[k], tp) for k in range(1, n_ep)]
    peers += [(me, tp_peer[o]) for o in range(1, n_tp)]
    peers += [(ep_peer[k], 2 * y_peer[j] + core) for k in range(1, n_ep) for j in range(1, n_y)]
    barrier = announce(peers)
    hidden_load = pltpu.make_async_copy(hidden_hbm, hid, load_sem.at[0])
    hidden_load.start()
    small_loads = [
        pltpu.make_async_copy(source, target, small_sem.at[i])
        for i, (source, target) in enumerate(
            (
                (w_igate_t_hbm, w_igate_t),
                (w_fgate_t_hbm, w_fgate_t),
                (input_bias_hbm, input_bias),
                (forget_bias_hbm, forget_bias),
                (max_state_t_hbm, max_state_t),
                (head_gain_hbm, head_gain),
                (gain1_hbm, gain1),
                (gain2_hbm, gain2),
                (group_router_t_hbm, group_router_t),
                (expert_router_t_hbm, expert_router_t),
                (route_t_hbm, route_t),
            )
        )
    ]
    w_loads = [pltpu.make_async_copy(w, weights.at[i], load_sem.at[1 + i]) for i, w in enumerate((wq, wk, wv, wo))]
    mem_load = pltpu.make_async_copy(memory, mem_out, load_sem.at[5])
    out_load = pltpu.make_async_copy(w_out, wo_buf, load_sem.at[6])
    gate_load = pltpu.make_async_copy(w_gate.at[0], wg_buf, load_sem.at[7])
    up_load = pltpu.make_async_copy(w_up.at[0], wu_buf, load_sem.at[8])
    down_load = pltpu.make_async_copy(w_down.at[0], wd_buf, load_sem.at[9])
    for load in small_loads + w_loads + [mem_load, out_load, gate_load, up_load, down_load]:
        load.start()
    hidden_load.wait()
    pl.semaphore_wait(barrier, len(peers))

    spreads = {}
    for k in far_first:
        columns = pl.ds(pl.multiple_of(ep_peer[k] * depth, depth), depth)
        spreads[k] = begin(remote(hid.at[:, columns], spread.at[k], h_send.at[k], h_recv.at[k], (ep_peer[k], tp)))
    spread[0] = hid[:, pl.ds(pl.multiple_of(me * depth, depth), depth)]
    for load in small_loads:
        load.wait()
    gate_w[...] = jnp.zeros_like(gate_w)
    in_rows = w_igate_t[...].astype(jnp.float32)
    forget_rows = w_fgate_t[...].astype(jnp.float32)
    for part in range(3):
        gate_w[2 * heads * part : 2 * heads * part + heads] = in_rows
        gate_w[2 * heads * part + heads : 2 * heads * (part + 1)] = forget_rows
    gate_half = gate_w[...].astype(jnp.bfloat16)

    mem_load.wait()

    def convert(b, carry):
        for h in range(heads):
            mem_half[h, pl.ds(pl.multiple_of(b * DH, DH), DH), :] = mem_out[b, pl.ds(h, DH, stride=heads), :].astype(
                jnp.bfloat16
            )
        return carry

    lax.fori_loop(0, rows, convert, 0)
    i_row = lax.broadcasted_iota(jnp.int32, (rows, rows), 0)
    i_col = lax.broadcasted_iota(jnp.int32, (rows, rows), 1)
    eye = i_row == i_col
    spread_row = lambda row: jnp.broadcast_to(row, (rows, rows))
    to_column = lambda row: jnp.sum(jnp.where(eye, spread_row(row), 0.0), 1, keepdims=True)
    to_row = lambda column: jnp.sum(jnp.where(eye, jnp.broadcast_to(column, (rows, rows)), 0.0), 0, keepdims=True)
    first_row = route_t[0:1, :].astype(jnp.float32)
    second_row = route_t[1:2, :].astype(jnp.float32)
    group_row = lax.shift_right_logical(route_t[0:1, :], GROUP_SIZE.bit_length() - 1).astype(jnp.float32)
    group_column = to_column(group_row)
    alike = jnp.broadcast_to(group_column, (rows, rows)) == spread_row(group_row)
    place_row = group_row * block + jnp.sum(jnp.where(alike & (i_row < i_col), 1.0, 0.0), 0, keepdims=True)
    place_column = to_column(place_row)
    perm_mask = spread_row(place_row) == i_row.astype(jnp.float32)
    perm = jnp.where(perm_mask, 1.0, 0.0).astype(jnp.bfloat16)
    back_mask = jnp.broadcast_to(place_column, (rows, rows)) == i_col.astype(jnp.float32)
    perm_back = jnp.where(back_mask, 1.0, 0.0).astype(jnp.bfloat16)
    first = jnp.sum(jnp.where(perm_mask, spread_row(first_row), 0.0), 1, keepdims=True)
    second = jnp.sum(jnp.where(perm_mask, spread_row(second_row), 0.0), 1, keepdims=True)
    hidden_sum = jnp.sum(dot32(perm, hid[...]), 1, keepdims=True)
    hidden_share = dot32(perm, hid[:, share_of(tp)])

    for load in w_loads:
        load.wait()
    for k in near_first:
        spreads[k].wait_recv()
    lhs = spread[...].reshape(n_ep * rows, depth)

    quad = GROUP_SIZE
    far_quads = range(1, n_ep // quad)
    bounds = [(0, cols), (cols, 2 * cols + DH), (2 * cols + DH, 3 * cols + DH), (3 * cols + DH, 4 * cols + DH)]
    cut = bounds[1][1]
    collected = [{} for _ in range(4)]
    arrivals = [{} for _ in range(4)]
    for i in range(4):
        part = dot32(lhs, weights[i])
        if i == 1:
            high, middle, low = three_parts(dot_t(lhs, gate_half))
            lane = lax.broadcasted_iota(jnp.int32, high.shape, 1)
            extra = jnp.where(lane < 2 * heads, high, jnp.where(lane < 4 * heads, middle, low))
            part = jnp.concatenate([part, extra], 1)
        span = slice(*bounds[i])
        proj_send[:, :, span] = part.astype(jnp.bfloat16).reshape(n_ep, rows, part.shape[1])
        proj_own[:, span] = part[:rows]
        for f in far_quads:
            far_own[f - 1, :, span] = part[f * quad * rows : (f * quad + 1) * rows]
        for f in far_quads:
            for j in range(quad - 1, 0, -1):
                collected[i][f, j] = begin(
                    remote(
                        proj_send.at[f * quad + j, :, span],
                        far_recv.at[f - 1, j - 1, :, span],
                        f_send.at[i, f - 1, j - 1],
                        f_recv.at[i, f - 1, j - 1],
                        (ep_peer[j], tp),
                    )
                )
    for i in range(4):
        span = slice(*bounds[i])
        for j in range(quad - 1, 0, -1):
            arrivals[i][j] = begin(
                remote(
                    proj_send.at[j, :, span], proj_recv.at[j, :, span], p_send.at[i, j], p_recv.at[i, j], (ep_peer[j], tp)
                )
            )
    crossed = [{} for _ in range(4)]
    for i in range(4):
        span = slice(*bounds[i])
        for f in far_quads:
            summed = far_own[f - 1, :, span]
            for j in range(1, quad):
                collected[i][f, j].wait_recv()
                summed += far_recv[f - 1, j - 1, :, span].astype(jnp.float32)
            if i < 2:
                source, target = cross_send.at[f - 1, :, span], cross_recv.at[f - 1, :, span]
                cross_send[f - 1, :, span] = summed
            else:
                span2 = slice(span.start - cut, span.stop - cut)
                source, target = cross_send2.at[f - 1, :, span2], cross_recv2.at[f - 1, :, span2]
                cross_send2[f - 1, :, span2] = summed.astype(jnp.bfloat16)
            crossed[i][f] = begin(
                remote(source, target, c_send.at[i, f - 1], c_recv.at[i, f - 1], (ep_peer[f * quad], tp))
            )

    def total(i):
        span = slice(*bounds[i])
        result = proj_own[:, span]
        for j in range(1, quad):
            arrivals[i][j].wait_recv()
            result += proj_recv[j, :, span].astype(jnp.float32)
        for f in far_quads:
            crossed[i][f].wait_recv()
            if i < 2:
                result += cross_recv[f - 1, :, span]
            else:
                result += cross_recv2[f - 1, :, span.start - cut : span.stop - cut].astype(jnp.float32)
        return result

    queries = total(0)
    read_old = []
    for h in range(heads):
        query = queries[:, h * DH : (h + 1) * DH]
        high = query.astype(jnp.bfloat16).astype(jnp.float32)
        both = jnp.concatenate([high, query - high], 0)
        row_of = lax.rem(lax.broadcasted_iota(jnp.int32, both.shape, 0), rows)
        spread_query = [jnp.where(row_of == b, both, 0.0).astype(jnp.bfloat16) for b in range(rows)]
        read = dot32(jnp.concatenate(spread_query, 1), mem_half[h])
        read_old.append(read[:rows] + read[rows:])
    second_total = total(1)
    keys = second_total[:, :cols] * DH ** (-0.5)
    gates = second_total[:, cols:]
    gates = gates + pltpu.roll(gates, DH - 2 * heads, 1) + pltpu.roll(gates, DH - 4 * heads, 1)
    scores = []
    for h in range(heads):
        span = slice(h * DH, (h + 1) * DH)
        scores.append(jnp.sum(queries[:, span] * keys[:, span], 1, keepdims=True))
    values = total(2)
    value_buf[...] = values
    last = total(3)
    mixed = []
    for h in range(heads):
        span = slice(h * DH, (h + 1) * DH)
        log_input = gates[:, h : h + 1] + input_bias[0:1, h : h + 1]
        forget = gates[:, heads + h : heads + h + 1] + forget_bias[0:1, h : h + 1]
        log_forget = jnp.minimum(forget, 0.0) - jnp.log1p(jnp.exp(-jnp.abs(forget)))
        carried = log_forget + to_column(max_state_t[h : h + 1, :])
        new_max = jnp.maximum(carried, log_input)
        keep = jnp.exp(carried - new_max)
        write = jnp.exp(log_input - new_max)
        max_out[h : h + 1, :] = to_row(new_max)
        keep_buf[h] = jnp.broadcast_to(keep, (rows, DH))
        write_keys[h * rows : (h + 1) * rows] = write * keys[:, span]
        readout = scores[h] * write * values[:, span] + keep * read_old[h]
        scaled = readout * lax.rsqrt(jnp.mean(readout * readout, -1, keepdims=True) + 1e-06)
        mixed.append((scaled * head_gain[:, span] * jax.nn.sigmoid(last[:, span])).astype(jnp.bfloat16))
    mixed_sorted = dot32(perm, jnp.concatenate(mixed, 1)).astype(jnp.bfloat16)

    out_load.wait()
    mixes = []
    partial_sum = jnp.zeros((rows, 1), jnp.float32)
    order = [o for o in range(1, n_tp)] + [0]
    for o in order:
        part = dot32(mixed_sorted, wo_buf[:, share_of(tp_peer[o])]).astype(jnp.bfloat16)
        mix_send[o] = part
        partial_sum += jnp.sum(part.astype(jnp.float32), 1, keepdims=True)
        if o:
            mixes.append(begin(remote(mix_send.at[o], mix_recv.at[o], m_send.at[o], m_recv.at[o], (me, tp_peer[o]))))
    high, middle, low = three_parts(partial_sum)
    lane = lax.broadcasted_iota(jnp.int32, (rows, DH), 1)
    parts = jnp.where(lane == 0, high, jnp.where(lane == 1, middle, jnp.where(lane == 2, low, 0.0)))
    sum_send[...] = parts.astype(jnp.bfloat16)
    sums = [
        begin(remote(sum_send, sum_recv.at[o], u_send.at[o], u_recv.at[o], (me, tp_peer[o]))) for o in range(1, n_tp)
    ]
    joined = res_alpha * hidden_share + mix_send[0].astype(jnp.float32)
    row_sum = res_alpha * hidden_sum + partial_sum
    for copy in mixes + sums:
        copy.wait_recv()
    for o in range(1, n_tp):
        joined += mix_recv[o].astype(jnp.float32)
        row_sum += jnp.sum(sum_recv[o].astype(jnp.float32), 1, keepdims=True)
    centred = joined - row_sum / width
    scaled_rows = centred * gain1[:, share_of(tp)]
    for g in range(groups):
        row_send[g] = scaled_rows[g * block : (g + 1) * block].astype(jnp.bfloat16)
    row_copies = {}
    for k in far_first + [0]:
        for j in range(n_y - 1, -1, -1):
            if k or j:
                row_copies[j, k] = begin(
                    remote(
                        row_send.at[lax.div(ep_peer[k], GROUP_SIZE)],
                        arrived.at[j, k],
                        a_send.at[j, k],
                        a_recv.at[j, k],
                        (ep_peer[k], 2 * y_peer[j] + core),
                    )
                )
    arrived[0, 0] = row_send[lax.div(me, GROUP_SIZE)]

    experts = expert_router_t.shape[0]
    expert_part = jnp.zeros((rows, experts), jnp.float32)
    group_part = jnp.zeros((rows, groups), jnp.float32)
    for piece in three_parts(scaled_rows):
        half = piece.astype(jnp.bfloat16)
        expert_part += dot_t(half, expert_router_t[:, share_of(tp)])
        group_part += dot_t(half, group_router_t[:, share_of(tp)])
    stat_send[...] = jnp.zeros_like(stat_send)
    stat_send[:, 0:experts] = expert_part
    stat_send[:, experts : experts + groups] = group_part
    stat_send[:, experts + groups : experts + groups + 1] = jnp.sum(centred * centred, 1, keepdims=True)
    stats = [
        begin(remote(stat_send, stat_recv.at[o], s_send.at[o], s_recv.at[o], (me, tp_peer[o]))) for o in range(1, n_tp)
    ]

    keys_t = write_keys[...].T
    for b in range(rows):
        for h in range(heads):
            old = mem_out[b, pl.ds(h, DH, stride=heads), :]
            column = keys_t[:, h * rows + b : h * rows + b + 1]
            value = value_buf[b : b + 1, h * DH : (h + 1) * DH]
            mem_out[b, pl.ds(h, DH, stride=heads), :] = keep_buf[h, b : b + 1, :] * old + column * value

    stat_total = stat_send[...]
    for o in range(1, n_tp):
        stats[o - 1].wait_recv()
        stat_total += stat_recv[o]
    row_scale = lax.rsqrt(stat_total[:, experts + groups : experts + groups + 1] / width + 1e-05)
    logits = stat_total * row_scale
    lanes = lax.broadcasted_iota(jnp.int32, logits.shape, 1).astype(jnp.float32)
    pick = lambda index: jnp.sum(jnp.where(lanes == index, logits, 0.0), 1, keepdims=True)
    first_logit = pick(first)
    second_logit = pick(second)
    group_gate = jax.nn.sigmoid(pick(experts + jnp.floor(first / GROUP_SIZE)))
    weight1 = group_gate * jax.nn.sigmoid(first_logit - second_logit)
    weight2 = group_gate * jax.nn.sigmoid(second_logit - first_logit)
    mid = (scaled_rows * row_scale).astype(jnp.bfloat16).astype(jnp.float32)
    for g in range(groups):
        span = slice(g * block, (g + 1) * block)
        for slot, column in enumerate((first, second, weight1, weight2)):
            weight_buf[slot, g] = jnp.broadcast_to(column[span], (block, DH))
        mid_buf[g] = res_alpha * mid[span]

    passed = {}
    for k in [0] + near_first:
        for j in range(n_y):
            if k or j:
                row_copies[j, k].wait_recv()
        passed[k] = begin(remote(arrived.at[:, k], arrived2.at[:, k], b_send.at[k], b_recv.at[k], partner))
    gate_load.wait()
    up_load.wait()
    count = n_ep * block
    gate_pre = jnp.zeros((count, wg_buf.shape[1]), jnp.float32)
    up_pre = jnp.zeros((count, wg_buf.shape[1]), jnp.float32)
    squares = jnp.zeros((count, DH), jnp.float32)
    for side, source in enumerate((arrived, arrived2)):
        if side:
            for k in range(n_ep):
                passed[k].wait_recv()
        for j in range(n_y):
            place = share_of(2 * y_from[j] + (1 - core if side else core))
            tokens32 = source[j].astype(jnp.float32).reshape(count, share)
            tokens = tokens32.astype(jnp.bfloat16)
            gate_pre += dot32(tokens, wg_buf[place, :])
            up_pre += dot32(tokens, wu_buf[place, :])
            plain = tokens32 / gain1[:, place]
            plain = plain * plain
            for c in range(share // DH):
                squares += plain[:, c * DH : (c + 1) * DH]
    token_scale = lax.rsqrt(jnp.sum(squares, 1, keepdims=True) / width + 1e-05)
    gate_pre *= token_scale
    units = (gate_pre * jax.nn.sigmoid(gate_pre) * (up_pre * token_scale)).astype(jnp.bfloat16)

    down_load.wait()
    downs = {}
    for j in range(n_y - 1, -1, -1):
        down_send[j] = dot32(units, wd_buf[:, share_of(2 * y_peer[j] + 1 - core)]).astype(jnp.bfloat16)
        downs[j] = begin(remote(down_send.at[j], down_recv.at[j], d_send.at[j], d_recv.at[j], partner))
    returns = {}
    own = {j: dot32(units, wd_buf[:, share_of(2 * y_peer[j] + core)]) for j in range(n_y - 1, -1, -1)}
    for j in range(n_y - 1, -1, -1):
        downs[j].wait_recv()
        result = own[j] + down_recv[j].astype(jnp.float32)
        for k in far_first + [0]:
            ret_send[j, k] = result[k * block : (k + 1) * block].astype(jnp.bfloat16)
            if k or j:
                returns[j, k] = begin(
                    remote(
                        ret_send.at[j, k],
                        ret_recv.at[j, k],
                        r_send.at[j, k],
                        r_recv.at[j, k],
                        (ep_peer[k], 2 * y_peer[j] + core),
                    )
                )
    for piece in range(groups):
        g = flip(lax.div(me, GROUP_SIZE), piece)
        gathered = mid_buf[g]
        for k in range(piece * GROUP_SIZE, (piece + 1) * GROUP_SIZE):
            expert = ep_peer[k].astype(jnp.float32)
            weight = jnp.where(weight_buf[0, g] == expert, weight_buf[2, g], 0.0)
            weight += jnp.where(weight_buf[1, g] == expert, weight_buf[3, g], 0.0)
            result = jnp.zeros((block, share), jnp.float32)
            for j in range(n_y):
                if k or j:
                    returns[j, k].wait_recv()
                result += (ret_recv[j, k] if k or j else ret_send[0, 0]).astype(jnp.float32)
            gathered += weight[:, 0:1] * result
        mid_buf[g] = gathered
    joined = mid_buf[...].reshape(rows, share)
    row_sum = jnp.sum(joined, -1, keepdims=True)
    square_sum = jnp.sum(joined * joined, -1, keepdims=True)
    stat2_send[...] = jnp.where(lane == 0, row_sum, square_sum)
    copies = [
        begin(remote(stat2_send, stat2_recv.at[o], t_send.at[o], t_recv.at[o], (me, tp_peer[o])))
        for o in range(1, n_tp)
    ]
    for o in range(1, n_tp):
        copies[o - 1].wait_recv()
        row_sum += stat2_recv[o][:, 0:1]
        square_sum += stat2_recv[o][:, 1:2]
    row_mean = row_sum / width
    row_var = square_sum / width - row_mean * row_mean
    result = ((joined - row_mean) * lax.rsqrt(row_var + 1e-05) * gain2[...]).astype(jnp.bfloat16)
    out_ref[...] = dot32(perm_back, result).astype(jnp.bfloat16)
    for copy in started:
        copy.wait_send()


def layer(n_ep, n_tp, groups, *operands):
    hidden, wq, _, _, _, memory, w_out, w_gate, _, w_down = operands[:10]
    rows, width = hidden.shape
    heads = memory.shape[1] // DH
    depth, cols = wq.shape
    share = width // n_tp
    block = rows // groups
    n_y = n_tp // 2
    half, full = jnp.bfloat16, jnp.float32
    vmem = pl.BlockSpec(memory_space=pltpu.VMEM)
    anywhere = pl.BlockSpec(memory_space=pl.ANY)
    dma = pltpu.SemaphoreType.DMA
    count = n_ep * block
    wide = 4 * cols + DH
    n_far = n_ep // GROUP_SIZE - 1
    return pl.pallas_call(
        functools.partial(layer_kernel, n_ep, n_tp, groups),
        out_shape=(
            pltpu.VMEM((rows, share), half),
            pltpu.VMEM(memory.shape, full),
            pltpu.VMEM((heads, rows), full),
        ),
        in_specs=[anywhere] * len(operands),
        out_specs=(vmem, vmem, vmem),
        scratch_shapes=[pltpu.VMEM(x.shape, x.dtype) for x in operands[10:]]
        + [
            pltpu.VMEM((rows, width), half),
            pltpu.VMEM((4, depth, cols), half),
            pltpu.VMEM(w_out.shape, half),
            pltpu.VMEM(w_gate.shape[1:], half),
            pltpu.VMEM(w_gate.shape[1:], half),
            pltpu.VMEM(w_down.shape[1:], half),
            pltpu.VMEM((heads, rows * DH, DH), half),
            pltpu.VMEM((DH, depth), full),
            pltpu.VMEM((n_ep, rows, depth), half),
            pltpu.VMEM((n_ep, rows, wide), half),
            pltpu.VMEM((n_ep, rows, wide), half),
            pltpu.VMEM((rows, wide), full),
            pltpu.VMEM((n_far, rows, wide), full),
            pltpu.VMEM((n_far, GROUP_SIZE - 1, rows, wide), half),
            pltpu.VMEM((n_far, rows, 2 * cols + DH), full),
            pltpu.VMEM((n_far, rows, 2 * cols + DH), full),
            pltpu.VMEM((n_far, rows, 2 * cols), half),
            pltpu.VMEM((n_far, rows, 2 * cols), half),
            pltpu.VMEM((heads * rows, DH), full),
            pltpu.VMEM((heads, rows, DH), full),
            pltpu.VMEM((rows, cols), full),
            pltpu.VMEM((n_tp, rows, share), half),
            pltpu.VMEM((n_tp, rows, share), half),
            pltpu.VMEM((rows, DH), half),
            pltpu.VMEM((n_tp, rows, DH), half),
            pltpu.VMEM((groups, block, share), half),
            pltpu.VMEM((n_y, n_ep, block, share), half),
            pltpu.VMEM((n_y, n_ep, block, share), half),
            pltpu.VMEM((rows, DH), full),
            pltpu.VMEM((n_tp, rows, DH), full),
            pltpu.VMEM((4, groups, block, DH), full),
            pltpu.VMEM((groups, block, share), full),
            pltpu.VMEM((n_y, count, share), half),
            pltpu.VMEM((n_y, count, share), half),
            pltpu.VMEM((n_y, n_ep, block, share), half),
            pltpu.VMEM((n_y, n_ep, block, share), half),
            pltpu.VMEM((rows, DH), full),
            pltpu.VMEM((n_tp, rows, DH), full),
            dma((10,)),
            dma((len(operands) - 10,)),
            dma((n_ep,)),
            dma((n_ep,)),
            dma((4, n_ep)),
            dma((4, n_ep)),
            dma((4, n_far, GROUP_SIZE - 1)),
            dma((4, n_far, GROUP_SIZE - 1)),
            dma((4, n_far)),
            dma((4, n_far)),
            dma((n_tp,)),
            dma((n_tp,)),
            dma((n_tp,)),
            dma((n_tp,)),
            dma((n_y, n_ep)),
            dma((n_y, n_ep)),
            dma((n_ep,)),
            dma((n_ep,)),
            dma((n_tp,)),
            dma((n_tp,)),
            dma((n_y,)),
            dma((n_y,)),
            dma((n_y, n_ep)),
            dma((n_y, n_ep)),
            dma((n_tp,)),
            dma((n_tp,)),
        ],
        compiler_params=pltpu.CompilerParams(
            collective_id=0, has_side_effects=True, vmem_limit_bytes=VMEM_LIMIT
        ),
        name="layer",
    )(*operands)


def store_kernel(result, memory, new_max, out_ref, mem_out, max_out, sems):
    copies = [
        pltpu.make_async_copy(source, target, sems.at[i])
        for i, (source, target) in enumerate(((memory, mem_out), (result, out_ref), (new_max, max_out)))
    ]
    for copy in copies:
        copy.start()
    for copy in copies:
        copy.wait()


def store(*operands):
    anywhere = pl.BlockSpec(memory_space=pl.ANY)
    return pl.pallas_call(
        store_kernel,
        out_shape=tuple(jax.ShapeDtypeStruct(x.shape, x.dtype) for x in operands),
        in_specs=[anywhere] * 3,
        out_specs=(anywhere,) * 3,
        scratch_shapes=[pltpu.SemaphoreType.DMA((3,))],
        compiler_params=pltpu.CompilerParams(vmem_limit_bytes=1 << 20),
        name="store",
    )(*operands)


def kernel_body(
    hidden_in,
    w_query,
    w_key,
    w_value,
    w_outgate,
    w_igate,
    w_fgate,
    input_bias,
    forget_bias,
    mem_state,
    max_state,
    head_gain,
    w_output,
    first_gain,
    w_group_router,
    w_expert_router,
    expert_route,
    w_expgate,
    w_expup,
    w_expdown,
    second_gain,
):
    n_ep, n_tp = lax.axis_size("ep"), lax.axis_size("tp")
    rows, heads, flat = mem_state.shape
    groups = w_group_router.shape[1]
    memory = mem_state.reshape(rows, heads, DH, DH).transpose(0, 2, 1, 3).reshape(rows, DH * heads, DH)
    results = layer(
        n_ep,
        n_tp,
        groups,
        hidden_in,
        w_query,
        w_key,
        w_value,
        w_outgate,
        memory,
        w_output,
        w_expgate,
        w_expup,
        w_expdown,
        w_igate.T,
        w_fgate.T,
        input_bias[None],
        forget_bias[None],
        max_state.T,
        head_gain[None],
        first_gain[None],
        second_gain[None],
        w_group_router.T,
        w_expert_router.T,
        expert_route.T,
    )
    hidden_out, memory_next, max_next = store(*results)
    memory_next = memory_next.reshape(rows, DH, heads, DH).transpose(0, 2, 1, 3).reshape(rows, heads, flat)
    return (hidden_out, memory_next, max_next.T)


def either_body(*operands):
    hidden_in, w_query, group_router, experts = operands[0], operands[1], operands[14], operands[17]
    rows, width = hidden_in.shape
    n_ep, n_tp = lax.axis_size("ep"), lax.axis_size("tp")
    groups = group_router.shape[1]
    block, odd_rows = divmod(rows, groups)
    aligned = rows % 16 == 0 and block % 8 == 0 and odd_rows == 0 and experts.shape[0] == 1
    aligned = aligned and w_query.shape[0] % DH == 0 and width // n_tp % DH == 0
    aligned = aligned and n_tp % 2 == 0 and n_ep & (n_ep - 1) == 0 and n_ep == groups * GROUP_SIZE and groups > 1
    return (kernel_body if aligned else body)(*operands)


def solution(mesh):
    return jax.shard_map(
        either_body,
        mesh=mesh,
        in_specs=(
            P("ep", None),
            P("ep", "tp"),
            P("ep", "tp"),
            P("ep", "tp"),
            P("ep", "tp"),
            P("ep", "tp"),
            P("ep", "tp"),
            P("tp"),
            P("tp"),
            P("ep", "tp", None),
            P("ep", "tp"),
            P("tp"),
            P("tp", None),
            P(),
            P(),
            P(),
            P("ep", None),
            P("ep", None, "tp"),
            P("ep", None, "tp"),
            P("ep", "tp", None),
            P("tp"),
        ),
        out_specs=(P("ep", "tp"), P("ep", "tp", None), P("ep", "tp")),
        check_vma=False,
    )
```

```python
import functools

import jax
import jax.numpy as jnp
from jax import lax
from jax.experimental import pallas as pl
from jax.experimental.pallas import tpu as pltpu
from jax.sharding import PartitionSpec as P

D = 4096
DH = 128
GROUP_SIZE = 4
MESH = pl.DeviceIdType.MESH


res_alpha = 8.0**0.25


def layer_norm(values, gain):
    row_mean = jnp.mean(values, -1, keepdims=True)
    row_var = jnp.mean(values * values, -1, keepdims=True) - row_mean * row_mean
    return (values - row_mean) * lax.rsqrt(row_var + 1e-05) * gain


def mlstm_step(queries, keys_scaled, values, log_input, log_forget, memory, stabilizer):
    new_max = jnp.maximum(log_forget + stabilizer, log_input)
    keep_old = jnp.exp(log_forget + stabilizer - new_max)
    write_new = jnp.exp(log_input - new_max)
    scores = jnp.sum(queries * keys_scaled, -1) * write_new
    read_old = jnp.einsum("bhd,bhde->bhe", queries, memory, precision=lax.Precision.HIGHEST)
    readout = scores[..., None] * values + keep_old[..., None] * read_old
    memory_next = (
        keep_old[..., None, None] * memory
        + write_new[..., None, None] * keys_scaled[..., :, None] * values[..., None, :]
    )
    return (readout, memory_next, new_max)


def head_mix(readout, head_gain, out_pre):
    scaled = readout * lax.rsqrt(jnp.mean(readout * readout, -1, keepdims=True) + 1e-06)
    flat_heads = scaled.reshape(scaled.shape[0], -1)
    return (flat_heads * head_gain * jax.nn.sigmoid(out_pre)).astype(jnp.bfloat16)


def route_weights(mid_float, w_group_router, w_expert_router, expert_route):
    group_logits = jnp.dot(
        mid_float, w_group_router.astype(jnp.float32), precision=lax.Precision.HIGHEST
    )
    expert_logits = jnp.dot(
        mid_float, w_expert_router.astype(jnp.float32), precision=lax.Precision.HIGHEST
    )
    first_expert = expert_route[:, 0]
    second_expert = expert_route[:, 1]
    expert_ids = lax.broadcasted_iota(jnp.int32, expert_logits.shape, 1)
    group_ids = lax.broadcasted_iota(jnp.int32, group_logits.shape, 1)
    first_logit = jnp.sum(jnp.where(expert_ids == first_expert[:, None], expert_logits, 0.0), -1)
    second_logit = jnp.sum(jnp.where(expert_ids == second_expert[:, None], expert_logits, 0.0), -1)
    group_pick = jnp.sum(
        jnp.where(group_ids == (first_expert // GROUP_SIZE)[:, None], group_logits, 0.0), -1
    )
    group_gate = jax.nn.sigmoid(group_pick)
    return (
        group_gate * jax.nn.sigmoid(first_logit - second_logit),
        group_gate * jax.nn.sigmoid(second_logit - first_logit),
    )


def slot_ranks(flat_routes, expert_total):
    onehot = (
        flat_routes[:, None]
        == lax.broadcasted_iota(jnp.int32, (flat_routes.shape[0], expert_total), 1)
    ).astype(jnp.int32)
    running = jnp.cumsum(onehot, 0)
    return jnp.sum((running - 1) * onehot, -1)


def body(
    hidden_in,
    w_query,
    w_key,
    w_value,
    w_outgate,
    w_igate,
    w_fgate,
    input_bias,
    forget_bias,
    mem_state,
    max_state,
    head_gain,
    w_output,
    first_gain,
    w_group_router,
    w_expert_router,
    expert_route,
    w_expgate,
    w_expup,
    w_expdown,
    second_gain,
):
    own_rows, width = hidden_in.shape
    heads_here = mem_state.shape[1]
    head_width = heads_here * DH
    top_count = expert_route.shape[1]
    spread_rows = lax.all_to_all(hidden_in, "ep", split_axis=1, concat_axis=0, tiled=True)
    stacked_w = jnp.concatenate([w_query, w_key, w_value, w_outgate], 1)
    gate_w = jnp.concatenate([w_igate, w_fgate], 1)
    proj_terms = jnp.dot(spread_rows, stacked_w, preferred_element_type=jnp.float32)
    gate_terms = jnp.dot(spread_rows, gate_w, preferred_element_type=jnp.float32)
    projected, gate_sums = (
        lax.psum_scatter(proj_terms, "ep", scatter_dimension=0, tiled=True),
        lax.psum_scatter(gate_terms, "ep", scatter_dimension=0, tiled=True),
    )
    shaped = projected.reshape(own_rows, 4, heads_here, DH)
    queries = shaped[:, 0]
    keys_raw = shaped[:, 1]
    values = shaped[:, 2]
    out_pre = shaped[:, 3].reshape(own_rows, head_width)
    input_sum = gate_sums[:, :heads_here]
    forget_sum = gate_sums[:, heads_here:]
    keys_scaled = keys_raw * DH ** (-0.5)
    log_input = input_sum + input_bias
    log_forget = jax.nn.log_sigmoid(forget_sum + forget_bias)
    memory = mem_state.reshape(own_rows, heads_here, DH, DH)
    readout, memory_square, new_max = mlstm_step(
        queries, keys_scaled, values, log_input, log_forget, memory, max_state
    )
    memory_next = memory_square.reshape(own_rows, heads_here, DH * DH)
    mixed_heads = head_mix(readout, head_gain, out_pre)
    partial_mix = jnp.dot(mixed_heads, w_output, preferred_element_type=jnp.float32).astype(
        jnp.bfloat16
    )
    mix = lax.psum(partial_mix.astype(jnp.float32).astype(jnp.bfloat16), "tp").astype(jnp.float32)
    mid_float = layer_norm(res_alpha * hidden_in.astype(jnp.float32) + mix, first_gain)
    mid = mid_float.astype(jnp.bfloat16)
    first_weight, second_weight = route_weights(
        mid_float, w_group_router, w_expert_router, expert_route
    )
    expert_total = w_expgate.shape[0] * lax.axis_size("ep")
    capacity = 2 * own_rows * top_count // expert_total
    flat_routes = expert_route.reshape(-1)
    local_slot = flat_routes * capacity + slot_ranks(flat_routes, expert_total)
    share_width = width // lax.axis_size("tp")
    mid_share = lax.dynamic_slice_in_dim(mid, lax.axis_index("tp") * share_width, share_width, 1)
    buffer = (
        jnp.zeros((expert_total * capacity, width), jnp.bfloat16)
        .at[local_slot]
        .set(jnp.repeat(mid, top_count, 0))
    )
    arrived = lax.all_to_all(
        buffer.reshape(expert_total, capacity, width), "ep", split_axis=0, concat_axis=1, tiled=True
    )
    gate_pre = jnp.einsum("erd,edf->erf", arrived, w_expgate, preferred_element_type=jnp.float32)
    up_pre = jnp.einsum("erd,edf->erf", arrived, w_expup, preferred_element_type=jnp.float32)
    hidden_units = (jax.nn.silu(gate_pre) * up_pre).astype(jnp.bfloat16)
    down_terms = jnp.einsum(
        "erf,efd->erd", hidden_units, w_expdown, preferred_element_type=jnp.float32
    ).astype(jnp.bfloat16)
    expert_share = lax.psum_scatter(
        down_terms.astype(jnp.float32).astype(jnp.bfloat16), "tp", scatter_dimension=2, tiled=True
    )
    returned = lax.all_to_all(expert_share, "ep", split_axis=1, concat_axis=0, tiled=True)
    picked = returned.reshape(expert_total * capacity, share_width)[local_slot]
    picked = picked.astype(jnp.float32).reshape(own_rows, top_count, share_width)
    moe = first_weight[:, None] * picked[:, 0] + second_weight[:, None] * picked[:, 1]
    joined = res_alpha * mid_share.astype(jnp.float32) + moe
    row_sum, square_sum = lax.psum((jnp.sum(joined, -1), jnp.sum(joined * joined, -1)), "tp")
    row_mean = row_sum / D
    row_var = square_sum / D - row_mean * row_mean
    hidden_out = (
        (joined - row_mean[:, None]) * lax.rsqrt(row_var[:, None] + 1e-05) * second_gain
    ).astype(jnp.bfloat16)
    return (hidden_out, memory_next, new_max)


VMEM_LIMIT = 59 * 1024 * 1024


def announce(peers):
    barrier = pltpu.get_barrier_semaphore()
    for peer in peers:
        pl.semaphore_signal(barrier, inc=1, device_id=peer, device_id_type=MESH)
    return barrier


def remote(source, target, send_sem, recv_sem, peer):
    return pltpu.make_async_remote_copy(
        src_ref=source,
        dst_ref=target,
        send_sem=send_sem,
        recv_sem=recv_sem,
        device_id=peer,
        device_id_type=MESH,
    )


def flip(index, bits):
    result = index
    place = 1
    while place <= bits:
        if bits & place:
            result = result + place * (1 - 2 * lax.rem(lax.div(index, place), 2))
        place *= 2
    return result


def three_parts(value):
    high = value.astype(jnp.bfloat16).astype(jnp.float32)
    rest = value - high
    middle = rest.astype(jnp.bfloat16).astype(jnp.float32)
    return high, middle, rest - middle


def dot32(left, right):
    return jnp.dot(left, right, preferred_element_type=jnp.float32)


def dot_t(left, right):
    return lax.dot_general(left, right, (((1,), (1,)), ((), ())), preferred_element_type=jnp.float32)


def layer_kernel(
    n_ep,
    n_tp,
    groups,
    hidden_hbm,
    wq,
    wk,
    wv,
    wo,
    memory,
    w_out,
    w_gate,
    w_up,
    w_down,
    w_igate_t_hbm,
    w_fgate_t_hbm,
    input_bias_hbm,
    forget_bias_hbm,
    max_state_t_hbm,
    head_gain_hbm,
    gain1_hbm,
    gain2_hbm,
    group_router_t_hbm,
    expert_router_t_hbm,
    route_t_hbm,
    out_ref,
    mem_out,
    max_out,
    w_igate_t,
    w_fgate_t,
    input_bias,
    forget_bias,
    max_state_t,
    head_gain,
    gain1,
    gain2,
    group_router_t,
    expert_router_t,
    route_t,
    hid,
    weights,
    wo_buf,
    wg_buf,
    wu_buf,
    wd_buf,
    mem_half,
    gate_w,
    spread,
    proj_send,
    proj_recv,
    proj_own,
    far_own,
    far_recv,
    cross_send,
    cross_recv,
    cross_send2,
    cross_recv2,
    write_keys,
    keep_buf,
    value_buf,
    mix_send,
    mix_recv,
    sum_send,
    sum_recv,
    row_send,
    arrived,
    arrived2,
    stat_send,
    stat_recv,
    weight_buf,
    mid_buf,
    down_send,
    down_recv,
    ret_send,
    ret_recv,
    stat2_send,
    stat2_recv,
    load_sem,
    small_sem,
    h_send,
    h_recv,
    p_send,
    p_recv,
    f_send,
    f_recv,
    c_send,
    c_recv,
    m_send,
    m_recv,
    u_send,
    u_recv,
    a_send,
    a_recv,
    b_send,
    b_recv,
    s_send,
    s_recv,
    d_send,
    d_recv,
    r_send,
    r_recv,
    t_send,
    t_recv,
):
    me = lax.axis_index("ep")
    tp = lax.axis_index("tp")
    n_y = n_tp // 2
    y = lax.div(tp, 2)
    core = lax.rem(tp, 2)
    rows, width = hid.shape
    share = width // n_tp
    block = rows // groups
    heads = keep_buf.shape[0]
    depth, cols = wq.shape
    far_first = list(range(n_ep - 1, 0, -1))
    near_first = list(range(1, n_ep))
    ep_peer = [flip(me, k) for k in range(n_ep)]
    y_peer = [lax.rem(y + j, n_y) for j in range(n_y)]
    y_from = [lax.rem(y + n_y - j, n_y) for j in range(n_y)]
    tp_peer = [lax.rem(tp + o, n_tp) for o in range(n_tp)]
    partner = (me, 2 * y + 1 - core)

    def received(ref, sem):
        remote(ref, ref, sem, sem, partner).wait_recv()

    def sent(ref, sem):
        remote(ref, ref, sem, sem, partner).wait_send()

    def share_of(index):
        return pl.ds(pl.multiple_of(index * share, share), share)

    peers = [(ep_peer[k], tp) for k in range(1, n_ep)]
    peers += [(me, tp_peer[o]) for o in range(1, n_tp)]
    peers += [(ep_peer[k], 2 * y_peer[j] + core) for k in range(1, n_ep) for j in range(1, n_y)]
    barrier = announce(peers)
    hidden_load = pltpu.make_async_copy(hidden_hbm, hid, load_sem.at[0])
    hidden_load.start()
    small_loads = [
        pltpu.make_async_copy(source, target, small_sem.at[i])
        for i, (source, target) in enumerate(
            (
                (w_igate_t_hbm, w_igate_t),
                (w_fgate_t_hbm, w_fgate_t),
                (input_bias_hbm, input_bias),
                (forget_bias_hbm, forget_bias),
                (max_state_t_hbm, max_state_t),
                (head_gain_hbm, head_gain),
                (gain1_hbm, gain1),
                (gain2_hbm, gain2),
                (group_router_t_hbm, group_router_t),
                (expert_router_t_hbm, expert_router_t),
                (route_t_hbm, route_t),
            )
        )
    ]
    w_loads = [pltpu.make_async_copy(w, weights.at[i], load_sem.at[1]) for i, w in enumerate((wq, wk, wv, wo))]
    mem_load = pltpu.make_async_copy(memory, mem_out, load_sem.at[2])
    out_load = pltpu.make_async_copy(w_out, wo_buf, load_sem.at[3])
    gate_load = pltpu.make_async_copy(w_gate.at[0], wg_buf, load_sem.at[4])
    up_load = pltpu.make_async_copy(w_up.at[0], wu_buf, load_sem.at[5])
    down_load = pltpu.make_async_copy(w_down.at[0], wd_buf, load_sem.at[6])
    for load in small_loads + w_loads + [mem_load, out_load, gate_load, up_load, down_load]:
        load.start()
    hidden_load.wait()
    pl.semaphore_wait(barrier, len(peers))

    for k in far_first:
        columns = pl.ds(pl.multiple_of(ep_peer[k] * depth, depth), depth)
        remote(hid.at[:, columns], spread.at[k], h_send.at[0], h_recv.at[0], (ep_peer[k], tp)).start()
    spread[0] = hid[:, pl.ds(pl.multiple_of(me * depth, depth), depth)]
    for load in small_loads:
        load.wait()
    gate_w[...] = jnp.zeros_like(gate_w)
    in_rows = w_igate_t[...].astype(jnp.float32)
    forget_rows = w_fgate_t[...].astype(jnp.float32)
    for part in range(3):
        gate_w[2 * heads * part : 2 * heads * part + heads] = in_rows
        gate_w[2 * heads * part + heads : 2 * heads * (part + 1)] = forget_rows
    gate_half = gate_w[...].astype(jnp.bfloat16)

    mem_load.wait()

    def convert(b, carry):
        for h in range(heads):
            mem_half[h, pl.ds(pl.multiple_of(b * DH, DH), DH), :] = mem_out[b, pl.ds(h, DH, stride=heads), :].astype(
                jnp.bfloat16
            )
        return carry

    lax.fori_loop(0, rows, convert, 0)
    i_row = lax.broadcasted_iota(jnp.int32, (rows, rows), 0)
    i_col = lax.broadcasted_iota(jnp.int32, (rows, rows), 1)
    eye = i_row == i_col
    spread_row = lambda row: jnp.broadcast_to(row, (rows, rows))
    to_column = lambda row: jnp.sum(jnp.where(eye, spread_row(row), 0.0), 1, keepdims=True)
    to_row = lambda column: jnp.sum(jnp.where(eye, jnp.broadcast_to(column, (rows, rows)), 0.0), 0, keepdims=True)
    first_row = route_t[0:1, :].astype(jnp.float32)
    second_row = route_t[1:2, :].astype(jnp.float32)
    group_row = lax.shift_right_logical(route_t[0:1, :], GROUP_SIZE.bit_length() - 1).astype(jnp.float32)
    group_column = to_column(group_row)
    alike = jnp.broadcast_to(group_column, (rows, rows)) == spread_row(group_row)
    place_row = group_row * block + jnp.sum(jnp.where(alike & (i_row < i_col), 1.0, 0.0), 0, keepdims=True)
    place_column = to_column(place_row)
    perm_mask = spread_row(place_row) == i_row.astype(jnp.float32)
    perm = jnp.where(perm_mask, 1.0, 0.0).astype(jnp.bfloat16)
    back_mask = jnp.broadcast_to(place_column, (rows, rows)) == i_col.astype(jnp.float32)
    perm_back = jnp.where(back_mask, 1.0, 0.0).astype(jnp.bfloat16)
    first = jnp.sum(jnp.where(perm_mask, spread_row(first_row), 0.0), 1, keepdims=True)
    second = jnp.sum(jnp.where(perm_mask, spread_row(second_row), 0.0), 1, keepdims=True)
    hidden_sum = jnp.sum(dot32(perm, hid[...]), 1, keepdims=True)
    hidden_share = dot32(perm, hid[:, share_of(tp)])

    pltpu.make_async_copy(weights, weights, load_sem.at[1]).wait()
    received(spread.at[pl.ds(1, n_ep - 1)], h_recv.at[0])
    lhs = spread[...].reshape(n_ep * rows, depth)

    quad = GROUP_SIZE
    far_quads = range(1, n_ep // quad)
    bounds = [(0, cols), (cols, 2 * cols + DH), (2 * cols + DH, 3 * cols + DH), (3 * cols + DH, 4 * cols + DH)]
    cut = bounds[1][1]
    for i in range(4):
        part = dot32(lhs, weights[i])
        if i == 1:
            high, middle, low = three_parts(dot_t(lhs, gate_half))
            lane = lax.broadcasted_iota(jnp.int32, high.shape, 1)
            extra = jnp.where(lane < 2 * heads, high, jnp.where(lane < 4 * heads, middle, low))
            part = jnp.concatenate([part, extra], 1)
        span = slice(*bounds[i])
        proj_send[:, :, span] = part.astype(jnp.bfloat16).reshape(n_ep, rows, part.shape[1])
        proj_own[:, span] = part[:rows]
        for f in far_quads:
            far_own[f - 1, :, span] = part[f * quad * rows : (f * quad + 1) * rows]
        for f in far_quads:
            for j in range(quad - 1, 0, -1):
                remote(
                    proj_send.at[f * quad + j, :, span],
                    far_recv.at[f - 1, j - 1, :, span],
                    f_send.at[0],
                    f_recv.at[i],
                    (ep_peer[j], tp),
                ).start()
    for i in range(4):
        span = slice(*bounds[i])
        for j in range(quad - 1, 0, -1):
            remote(
                proj_send.at[j, :, span], proj_recv.at[j, :, span], p_send.at[0], p_recv.at[i], (ep_peer[j], tp)
            ).start()
    for i in range(4):
        span = slice(*bounds[i])
        received(far_recv.at[:, :, :, span], f_recv.at[i])
        for f in far_quads:
            summed = far_own[f - 1, :, span]
            for j in range(1, quad):
                summed += far_recv[f - 1, j - 1, :, span].astype(jnp.float32)
            if i < 2:
                source, target = cross_send.at[f - 1, :, span], cross_recv.at[f - 1, :, span]
                cross_send[f - 1, :, span] = summed
            else:
                span2 = slice(span.start - cut, span.stop - cut)
                source, target = cross_send2.at[f - 1, :, span2], cross_recv2.at[f - 1, :, span2]
                cross_send2[f - 1, :, span2] = summed.astype(jnp.bfloat16)
            remote(source, target, c_send.at[i // 2], c_recv.at[i], (ep_peer[f * quad], tp)).start()

    def total(i):
        span = slice(*bounds[i])
        result = proj_own[:, span]
        received(proj_recv.at[pl.ds(1, quad - 1), :, span], p_recv.at[i])
        if i < 2:
            received(cross_recv.at[:, :, span], c_recv.at[i])
        else:
            received(cross_recv2.at[:, :, slice(span.start - cut, span.stop - cut)], c_recv.at[i])
        for j in range(1, quad):
            result += proj_recv[j, :, span].astype(jnp.float32)
        for f in far_quads:
            if i < 2:
                result += cross_recv[f - 1, :, span]
            else:
                result += cross_recv2[f - 1, :, span.start - cut : span.stop - cut].astype(jnp.float32)
        return result

    queries = total(0)
    read_old = []
    for h in range(heads):
        query = queries[:, h * DH : (h + 1) * DH]
        high = query.astype(jnp.bfloat16).astype(jnp.float32)
        both = jnp.concatenate([high, query - high], 0)
        row_of = lax.rem(lax.broadcasted_iota(jnp.int32, both.shape, 0), rows)
        spread_query = [jnp.where(row_of == b, both, 0.0).astype(jnp.bfloat16) for b in range(rows)]
        read = dot32(jnp.concatenate(spread_query, 1), mem_half[h])
        read_old.append(read[:rows] + read[rows:])
    second_total = total(1)
    keys = second_total[:, :cols] * DH ** (-0.5)
    gates = second_total[:, cols:]
    gates = gates + pltpu.roll(gates, DH - 2 * heads, 1) + pltpu.roll(gates, DH - 4 * heads, 1)
    scores = []
    for h in range(heads):
        span = slice(h * DH, (h + 1) * DH)
        scores.append(jnp.sum(queries[:, span] * keys[:, span], 1, keepdims=True))
    values = total(2)
    value_buf[...] = values
    last = total(3)
    mixed = []
    for h in range(heads):
        span = slice(h * DH, (h + 1) * DH)
        log_input = gates[:, h : h + 1] + input_bias[0:1, h : h + 1]
        forget = gates[:, heads + h : heads + h + 1] + forget_bias[0:1, h : h + 1]
        log_forget = jnp.minimum(forget, 0.0) - jnp.log1p(jnp.exp(-jnp.abs(forget)))
        carried = log_forget + to_column(max_state_t[h : h + 1, :])
        new_max = jnp.maximum(carried, log_input)
        keep = jnp.exp(carried - new_max)
        write = jnp.exp(log_input - new_max)
        max_out[h : h + 1, :] = to_row(new_max)
        keep_buf[h] = jnp.broadcast_to(keep, (rows, DH))
        write_keys[h * rows : (h + 1) * rows] = write * keys[:, span]
        readout = scores[h] * write * values[:, span] + keep * read_old[h]
        scaled = readout * lax.rsqrt(jnp.mean(readout * readout, -1, keepdims=True) + 1e-06)
        mixed.append((scaled * head_gain[:, span] * jax.nn.sigmoid(last[:, span])).astype(jnp.bfloat16))
    mixed_sorted = dot32(perm, jnp.concatenate(mixed, 1)).astype(jnp.bfloat16)

    out_load.wait()
    partial_sum = jnp.zeros((rows, 1), jnp.float32)
    order = [o for o in range(1, n_tp)] + [0]
    for o in order:
        part = dot32(mixed_sorted, wo_buf[:, share_of(tp_peer[o])]).astype(jnp.bfloat16)
        mix_send[o] = part
        partial_sum += jnp.sum(part.astype(jnp.float32), 1, keepdims=True)
        if o:
            remote(mix_send.at[o], mix_recv.at[o], m_send.at[0], m_recv.at[0], (me, tp_peer[o])).start()
    high, middle, low = three_parts(partial_sum)
    lane = lax.broadcasted_iota(jnp.int32, (rows, DH), 1)
    parts = jnp.where(lane == 0, high, jnp.where(lane == 1, middle, jnp.where(lane == 2, low, 0.0)))
    sum_send[...] = parts.astype(jnp.bfloat16)
    others = pl.ds(1, n_tp - 1)
    for o in range(1, n_tp):
        remote(sum_send, sum_recv.at[o], u_send.at[0], u_recv.at[0], (me, tp_peer[o])).start()
    joined = res_alpha * hidden_share + mix_send[0].astype(jnp.float32)
    row_sum = res_alpha * hidden_sum + partial_sum
    received(mix_recv.at[others], m_recv.at[0])
    received(sum_recv.at[others], u_recv.at[0])
    for o in range(1, n_tp):
        joined += mix_recv[o].astype(jnp.float32)
        row_sum += jnp.sum(sum_recv[o].astype(jnp.float32), 1, keepdims=True)
    centred = joined - row_sum / width
    scaled_rows = centred * gain1[:, share_of(tp)]
    for g in range(groups):
        row_send[g] = scaled_rows[g * block : (g + 1) * block].astype(jnp.bfloat16)
    for k in far_first + [0]:
        for j in range(n_y - 1, -1, -1):
            if k or j:
                remote(
                    row_send.at[lax.div(ep_peer[k], GROUP_SIZE)],
                    arrived.at[j, k],
                    a_send.at[min(j, 1)],
                    a_recv.at[k],
                    (ep_peer[k], 2 * y_peer[j] + core),
                ).start()
    arrived[0, 0] = row_send[lax.div(me, GROUP_SIZE)]

    experts = expert_router_t.shape[0]
    expert_part = jnp.zeros((rows, experts), jnp.float32)
    group_part = jnp.zeros((rows, groups), jnp.float32)
    for piece in three_parts(scaled_rows):
        half = piece.astype(jnp.bfloat16)
        expert_part += dot_t(half, expert_router_t[:, share_of(tp)])
        group_part += dot_t(half, group_router_t[:, share_of(tp)])
    stat_send[...] = jnp.zeros_like(stat_send)
    stat_send[:, 0:experts] = expert_part
    stat_send[:, experts : experts + groups] = group_part
    stat_send[:, experts + groups : experts + groups + 1] = jnp.sum(centred * centred, 1, keepdims=True)
    for o in range(1, n_tp):
        remote(stat_send, stat_recv.at[o], s_send.at[0], s_recv.at[0], (me, tp_peer[o])).start()

    keys_t = write_keys[...].T
    for b in range(rows):
        for h in range(heads):
            old = mem_out[b, pl.ds(h, DH, stride=heads), :]
            column = keys_t[:, h * rows + b : h * rows + b + 1]
            value = value_buf[b : b + 1, h * DH : (h + 1) * DH]
            mem_out[b, pl.ds(h, DH, stride=heads), :] = keep_buf[h, b : b + 1, :] * old + column * value

    stat_total = stat_send[...]
    received(stat_recv.at[others], s_recv.at[0])
    for o in range(1, n_tp):
        stat_total += stat_recv[o]
    row_scale = lax.rsqrt(stat_total[:, experts + groups : experts + groups + 1] / width + 1e-05)
    logits = stat_total * row_scale
    lanes = lax.broadcasted_iota(jnp.int32, logits.shape, 1).astype(jnp.float32)
    pick = lambda index: jnp.sum(jnp.where(lanes == index, logits, 0.0), 1, keepdims=True)
    first_logit = pick(first)
    second_logit = pick(second)
    group_gate = jax.nn.sigmoid(pick(experts + jnp.floor(first / GROUP_SIZE)))
    weight1 = group_gate * jax.nn.sigmoid(first_logit - second_logit)
    weight2 = group_gate * jax.nn.sigmoid(second_logit - first_logit)
    mid = (scaled_rows * row_scale).astype(jnp.bfloat16).astype(jnp.float32)
    for g in range(groups):
        span = slice(g * block, (g + 1) * block)
        for slot, column in enumerate((first, second, weight1, weight2)):
            weight_buf[slot, g] = jnp.broadcast_to(column[span], (block, DH))
        mid_buf[g] = res_alpha * mid[span]

    for k in [0] + near_first:
        first_j = 0 if k else 1
        received(arrived.at[pl.ds(first_j, n_y - first_j), k], a_recv.at[k])
        remote(arrived.at[:, k], arrived2.at[:, k], b_send.at[0], b_recv.at[0], partner).start()
    gate_load.wait()
    up_load.wait()
    count = n_ep * block
    gate_pre = jnp.zeros((count, wg_buf.shape[1]), jnp.float32)
    up_pre = jnp.zeros((count, wg_buf.shape[1]), jnp.float32)
    squares = jnp.zeros((count, DH), jnp.float32)
    for side, source in enumerate((arrived, arrived2)):
        if side:
            received(arrived2, b_recv.at[0])
        for j in range(n_y):
            place = share_of(2 * y_from[j] + (1 - core if side else core))
            tokens32 = source[j].astype(jnp.float32).reshape(count, share)
            tokens = tokens32.astype(jnp.bfloat16)
            gate_pre += dot32(tokens, wg_buf[place, :])
            up_pre += dot32(tokens, wu_buf[place, :])
            plain = tokens32 / gain1[:, place]
            plain = plain * plain
            for c in range(share // DH):
                squares += plain[:, c * DH : (c + 1) * DH]
    token_scale = lax.rsqrt(jnp.sum(squares, 1, keepdims=True) / width + 1e-05)
    gate_pre *= token_scale
    units = (gate_pre * jax.nn.sigmoid(gate_pre) * (up_pre * token_scale)).astype(jnp.bfloat16)

    down_load.wait()
    for j in range(n_y - 1, -1, -1):
        down_send[j] = dot32(units, wd_buf[:, share_of(2 * y_peer[j] + 1 - core)]).astype(jnp.bfloat16)
        remote(down_send.at[j], down_recv.at[j], d_send.at[0], d_recv.at[j], partner).start()
    own = {j: dot32(units, wd_buf[:, share_of(2 * y_peer[j] + core)]) for j in range(n_y - 1, -1, -1)}
    for j in range(n_y - 1, -1, -1):
        received(down_recv.at[j], d_recv.at[j])
        result = own[j] + down_recv[j].astype(jnp.float32)
        for k in far_first + [0]:
            ret_send[j, k] = result[k * block : (k + 1) * block].astype(jnp.bfloat16)
            if k or j:
                remote(
                    ret_send.at[j, k],
                    ret_recv.at[j, k],
                    r_send.at[min(j, 1)],
                    r_recv.at[k],
                    (ep_peer[k], 2 * y_peer[j] + core),
                ).start()
    for piece in range(groups):
        g = flip(lax.div(me, GROUP_SIZE), piece)
        gathered = mid_buf[g]
        for k in range(piece * GROUP_SIZE, (piece + 1) * GROUP_SIZE):
            expert = ep_peer[k].astype(jnp.float32)
            weight = jnp.where(weight_buf[0, g] == expert, weight_buf[2, g], 0.0)
            weight += jnp.where(weight_buf[1, g] == expert, weight_buf[3, g], 0.0)
            first_j = 0 if k else 1
            received(ret_recv.at[pl.ds(first_j, n_y - first_j), k], r_recv.at[k])
            result = jnp.zeros((block, share), jnp.float32)
            for j in range(n_y):
                result += (ret_recv[j, k] if k or j else ret_send[0, 0]).astype(jnp.float32)
            gathered += weight[:, 0:1] * result
        mid_buf[g] = gathered
    joined = mid_buf[...].reshape(rows, share)
    row_sum = jnp.sum(joined, -1, keepdims=True)
    square_sum = jnp.sum(joined * joined, -1, keepdims=True)
    stat2_send[...] = jnp.where(lane == 0, row_sum, square_sum)
    for o in range(1, n_tp):
        remote(stat2_send, stat2_recv.at[o], t_send.at[0], t_recv.at[0], (me, tp_peer[o])).start()
    received(stat2_recv.at[others], t_recv.at[0])
    for o in range(1, n_tp):
        row_sum += stat2_recv[o][:, 0:1]
        square_sum += stat2_recv[o][:, 1:2]
    row_mean = row_sum / width
    row_var = square_sum / width - row_mean * row_mean
    result = ((joined - row_mean) * lax.rsqrt(row_var + 1e-05) * gain2[...]).astype(jnp.bfloat16)
    out_ref[...] = dot32(perm_back, result).astype(jnp.bfloat16)
    rest = pl.ds(1, n_ep - 1)
    for ref, sem in (
        (spread.at[rest], h_send.at[0]),
        (far_recv, f_send.at[0]),
        (proj_recv.at[pl.ds(1, quad - 1)], p_send.at[0]),
        (cross_send, c_send.at[0]),
        (cross_send2, c_send.at[1]),
        (mix_send.at[others], m_send.at[0]),
        (sum_recv.at[others], u_send.at[0]),
        (arrived.at[0, rest], a_send.at[0]),
        (arrived.at[pl.ds(1, n_y - 1)], a_send.at[1]),
        (stat_recv.at[others], s_send.at[0]),
        (arrived, b_send.at[0]),
        (down_send, d_send.at[0]),
        (ret_send.at[0, rest], r_send.at[0]),
        (ret_send.at[pl.ds(1, n_y - 1)], r_send.at[1]),
        (stat2_recv.at[others], t_send.at[0]),
    ):
        sent(ref, sem)


def layer(n_ep, n_tp, groups, *operands):
    hidden, wq, _, _, _, memory, w_out, w_gate, _, w_down = operands[:10]
    rows, width = hidden.shape
    heads = memory.shape[1] // DH
    depth, cols = wq.shape
    share = width // n_tp
    block = rows // groups
    n_y = n_tp // 2
    half, full = jnp.bfloat16, jnp.float32
    vmem = pl.BlockSpec(memory_space=pltpu.VMEM)
    anywhere = pl.BlockSpec(memory_space=pl.ANY)
    dma = pltpu.SemaphoreType.DMA
    count = n_ep * block
    wide = 4 * cols + DH
    n_far = n_ep // GROUP_SIZE - 1
    return pl.pallas_call(
        functools.partial(layer_kernel, n_ep, n_tp, groups),
        out_shape=(
            pltpu.VMEM((rows, share), half),
            pltpu.VMEM(memory.shape, full),
            pltpu.VMEM((heads, rows), full),
        ),
        in_specs=[anywhere] * len(operands),
        out_specs=(vmem, vmem, vmem),
        scratch_shapes=[pltpu.VMEM(x.shape, x.dtype) for x in operands[10:]]
        + [
            pltpu.VMEM((rows, width), half),
            pltpu.VMEM((4, depth, cols), half),
            pltpu.VMEM(w_out.shape, half),
            pltpu.VMEM(w_gate.shape[1:], half),
            pltpu.VMEM(w_gate.shape[1:], half),
            pltpu.VMEM(w_down.shape[1:], half),
            pltpu.VMEM((heads, rows * DH, DH), half),
            pltpu.VMEM((DH, depth), full),
            pltpu.VMEM((n_ep, rows, depth), half),
            pltpu.VMEM((n_ep, rows, wide), half),
            pltpu.VMEM((n_ep, rows, wide), half),
            pltpu.VMEM((rows, wide), full),
            pltpu.VMEM((n_far, rows, wide), full),
            pltpu.VMEM((n_far, GROUP_SIZE - 1, rows, wide), half),
            pltpu.VMEM((n_far, rows, 2 * cols + DH), full),
            pltpu.VMEM((n_far, rows, 2 * cols + DH), full),
            pltpu.VMEM((n_far, rows, 2 * cols), half),
            pltpu.VMEM((n_far, rows, 2 * cols), half),
            pltpu.VMEM((heads * rows, DH), full),
            pltpu.VMEM((heads, rows, DH), full),
            pltpu.VMEM((rows, cols), full),
            pltpu.VMEM((n_tp, rows, share), half),
            pltpu.VMEM((n_tp, rows, share), half),
            pltpu.VMEM((rows, DH), half),
            pltpu.VMEM((n_tp, rows, DH), half),
            pltpu.VMEM((groups, block, share), half),
            pltpu.VMEM((n_y, n_ep, block, share), half),
            pltpu.VMEM((n_y, n_ep, block, share), half),
            pltpu.VMEM((rows, DH), full),
            pltpu.VMEM((n_tp, rows, DH), full),
            pltpu.VMEM((4, groups, block, DH), full),
            pltpu.VMEM((groups, block, share), full),
            pltpu.VMEM((n_y, count, share), half),
            pltpu.VMEM((n_y, count, share), half),
            pltpu.VMEM((n_y, n_ep, block, share), half),
            pltpu.VMEM((n_y, n_ep, block, share), half),
            pltpu.VMEM((rows, DH), full),
            pltpu.VMEM((n_tp, rows, DH), full),
            dma((7,)),
            dma((len(operands) - 10,)),
            dma((1,)),
            dma((1,)),
            dma((1,)),
            dma((4,)),
            dma((1,)),
            dma((4,)),
            dma((2,)),
            dma((4,)),
            dma((1,)),
            dma((1,)),
            dma((1,)),
            dma((1,)),
            dma((2,)),
            dma((n_ep,)),
            dma((1,)),
            dma((1,)),
            dma((1,)),
            dma((1,)),
            dma((1,)),
            dma((n_y,)),
            dma((2,)),
            dma((n_ep,)),
            dma((1,)),
            dma((1,)),
        ],
        compiler_params=pltpu.CompilerParams(
            collective_id=0, has_side_effects=True, vmem_limit_bytes=VMEM_LIMIT
        ),
        name="layer",
    )(*operands)


def store_kernel(result, memory, new_max, out_ref, mem_out, max_out, sems):
    copies = [
        pltpu.make_async_copy(source, target, sems.at[i])
        for i, (source, target) in enumerate(((memory, mem_out), (result, out_ref), (new_max, max_out)))
    ]
    for copy in copies:
        copy.start()
    for copy in copies:
        copy.wait()


def store(*operands):
    anywhere = pl.BlockSpec(memory_space=pl.ANY)
    return pl.pallas_call(
        store_kernel,
        out_shape=tuple(jax.ShapeDtypeStruct(x.shape, x.dtype) for x in operands),
        in_specs=[anywhere] * 3,
        out_specs=(anywhere,) * 3,
        scratch_shapes=[pltpu.SemaphoreType.DMA((3,))],
        compiler_params=pltpu.CompilerParams(vmem_limit_bytes=1 << 20),
        name="store",
    )(*operands)


def kernel_body(
    hidden_in,
    w_query,
    w_key,
    w_value,
    w_outgate,
    w_igate,
    w_fgate,
    input_bias,
    forget_bias,
    mem_state,
    max_state,
    head_gain,
    w_output,
    first_gain,
    w_group_router,
    w_expert_router,
    expert_route,
    w_expgate,
    w_expup,
    w_expdown,
    second_gain,
):
    n_ep, n_tp = lax.axis_size("ep"), lax.axis_size("tp")
    rows, heads, flat = mem_state.shape
    groups = w_group_router.shape[1]
    memory = mem_state.reshape(rows, heads, DH, DH).transpose(0, 2, 1, 3).reshape(rows, DH * heads, DH)
    results = layer(
        n_ep,
        n_tp,
        groups,
        hidden_in,
        w_query,
        w_key,
        w_value,
        w_outgate,
        memory,
        w_output,
        w_expgate,
        w_expup,
        w_expdown,
        w_igate.T,
        w_fgate.T,
        input_bias[None],
        forget_bias[None],
        max_state.T,
        head_gain[None],
        first_gain[None],
        second_gain[None],
        w_group_router.T,
        w_expert_router.T,
        expert_route.T,
    )
    hidden_out, memory_next, max_next = store(*results)
    memory_next = memory_next.reshape(rows, DH, heads, DH).transpose(0, 2, 1, 3).reshape(rows, heads, flat)
    return (hidden_out, memory_next, max_next.T)


def either_body(*operands):
    hidden_in, w_query, group_router, experts = operands[0], operands[1], operands[14], operands[17]
    rows, width = hidden_in.shape
    n_ep, n_tp = lax.axis_size("ep"), lax.axis_size("tp")
    groups = group_router.shape[1]
    block, odd_rows = divmod(rows, groups)
    aligned = rows % 16 == 0 and block % 8 == 0 and odd_rows == 0 and experts.shape[0] == 1
    aligned = aligned and w_query.shape[0] % DH == 0 and width // n_tp % DH == 0
    aligned = aligned and n_tp % 2 == 0 and n_ep & (n_ep - 1) == 0 and n_ep == groups * GROUP_SIZE and groups > 1
    return (kernel_body if aligned else body)(*operands)


def solution(mesh):
    return jax.shard_map(
        either_body,
        mesh=mesh,
        in_specs=(
            P("ep", None),
            P("ep", "tp"),
            P("ep", "tp"),
            P("ep", "tp"),
            P("ep", "tp"),
            P("ep", "tp"),
            P("ep", "tp"),
            P("tp"),
            P("tp"),
            P("ep", "tp", None),
            P("ep", "tp"),
            P("tp"),
            P("tp", None),
            P(),
            P(),
            P(),
            P("ep", None),
            P("ep", None, "tp"),
            P("ep", None, "tp"),
            P("ep", "tp", None),
            P("tp"),
        ),
        out_specs=(P("ep", "tp"), P("ep", "tp", None), P("ep", "tp")),
        check_vma=False,
    )
```

```python
import functools

import jax
import jax.numpy as jnp
from jax import lax
from jax.experimental import pallas as pl
from jax.experimental.pallas import tpu as pltpu
from jax.sharding import PartitionSpec as P

D = 4096
DH = 128
GROUP_SIZE = 4
MESH = pl.DeviceIdType.MESH


res_alpha = 8.0**0.25


def layer_norm(values, gain):
    row_mean = jnp.mean(values, -1, keepdims=True)
    row_var = jnp.mean(values * values, -1, keepdims=True) - row_mean * row_mean
    return (values - row_mean) * lax.rsqrt(row_var + 1e-05) * gain


def mlstm_step(queries, keys_scaled, values, log_input, log_forget, memory, stabilizer):
    new_max = jnp.maximum(log_forget + stabilizer, log_input)
    keep_old = jnp.exp(log_forget + stabilizer - new_max)
    write_new = jnp.exp(log_input - new_max)
    scores = jnp.sum(queries * keys_scaled, -1) * write_new
    read_old = jnp.einsum("bhd,bhde->bhe", queries, memory, precision=lax.Precision.HIGHEST)
    readout = scores[..., None] * values + keep_old[..., None] * read_old
    memory_next = (
        keep_old[..., None, None] * memory
        + write_new[..., None, None] * keys_scaled[..., :, None] * values[..., None, :]
    )
    return (readout, memory_next, new_max)


def head_mix(readout, head_gain, out_pre):
    scaled = readout * lax.rsqrt(jnp.mean(readout * readout, -1, keepdims=True) + 1e-06)
    flat_heads = scaled.reshape(scaled.shape[0], -1)
    return (flat_heads * head_gain * jax.nn.sigmoid(out_pre)).astype(jnp.bfloat16)


def route_weights(mid_float, w_group_router, w_expert_router, expert_route):
    group_logits = jnp.dot(
        mid_float, w_group_router.astype(jnp.float32), precision=lax.Precision.HIGHEST
    )
    expert_logits = jnp.dot(
        mid_float, w_expert_router.astype(jnp.float32), precision=lax.Precision.HIGHEST
    )
    first_expert = expert_route[:, 0]
    second_expert = expert_route[:, 1]
    expert_ids = lax.broadcasted_iota(jnp.int32, expert_logits.shape, 1)
    group_ids = lax.broadcasted_iota(jnp.int32, group_logits.shape, 1)
    first_logit = jnp.sum(jnp.where(expert_ids == first_expert[:, None], expert_logits, 0.0), -1)
    second_logit = jnp.sum(jnp.where(expert_ids == second_expert[:, None], expert_logits, 0.0), -1)
    group_pick = jnp.sum(
        jnp.where(group_ids == (first_expert // GROUP_SIZE)[:, None], group_logits, 0.0), -1
    )
    group_gate = jax.nn.sigmoid(group_pick)
    return (
        group_gate * jax.nn.sigmoid(first_logit - second_logit),
        group_gate * jax.nn.sigmoid(second_logit - first_logit),
    )


def slot_ranks(flat_routes, expert_total):
    onehot = (
        flat_routes[:, None]
        == lax.broadcasted_iota(jnp.int32, (flat_routes.shape[0], expert_total), 1)
    ).astype(jnp.int32)
    running = jnp.cumsum(onehot, 0)
    return jnp.sum((running - 1) * onehot, -1)


def body(
    hidden_in,
    w_query,
    w_key,
    w_value,
    w_outgate,
    w_igate,
    w_fgate,
    input_bias,
    forget_bias,
    mem_state,
    max_state,
    head_gain,
    w_output,
    first_gain,
    w_group_router,
    w_expert_router,
    expert_route,
    w_expgate,
    w_expup,
    w_expdown,
    second_gain,
):
    own_rows, width = hidden_in.shape
    heads_here = mem_state.shape[1]
    head_width = heads_here * DH
    top_count = expert_route.shape[1]
    spread_rows = lax.all_to_all(hidden_in, "ep", split_axis=1, concat_axis=0, tiled=True)
    stacked_w = jnp.concatenate([w_query, w_key, w_value, w_outgate], 1)
    gate_w = jnp.concatenate([w_igate, w_fgate], 1)
    proj_terms = jnp.dot(spread_rows, stacked_w, preferred_element_type=jnp.float32)
    gate_terms = jnp.dot(spread_rows, gate_w, preferred_element_type=jnp.float32)
    projected, gate_sums = (
        lax.psum_scatter(proj_terms, "ep", scatter_dimension=0, tiled=True),
        lax.psum_scatter(gate_terms, "ep", scatter_dimension=0, tiled=True),
    )
    shaped = projected.reshape(own_rows, 4, heads_here, DH)
    queries = shaped[:, 0]
    keys_raw = shaped[:, 1]
    values = shaped[:, 2]
    out_pre = shaped[:, 3].reshape(own_rows, head_width)
    input_sum = gate_sums[:, :heads_here]
    forget_sum = gate_sums[:, heads_here:]
    keys_scaled = keys_raw * DH ** (-0.5)
    log_input = input_sum + input_bias
    log_forget = jax.nn.log_sigmoid(forget_sum + forget_bias)
    memory = mem_state.reshape(own_rows, heads_here, DH, DH)
    readout, memory_square, new_max = mlstm_step(
        queries, keys_scaled, values, log_input, log_forget, memory, max_state
    )
    memory_next = memory_square.reshape(own_rows, heads_here, DH * DH)
    mixed_heads = head_mix(readout, head_gain, out_pre)
    partial_mix = jnp.dot(mixed_heads, w_output, preferred_element_type=jnp.float32).astype(
        jnp.bfloat16
    )
    mix = lax.psum(partial_mix.astype(jnp.float32).astype(jnp.bfloat16), "tp").astype(jnp.float32)
    mid_float = layer_norm(res_alpha * hidden_in.astype(jnp.float32) + mix, first_gain)
    mid = mid_float.astype(jnp.bfloat16)
    first_weight, second_weight = route_weights(
        mid_float, w_group_router, w_expert_router, expert_route
    )
    expert_total = w_expgate.shape[0] * lax.axis_size("ep")
    capacity = 2 * own_rows * top_count // expert_total
    flat_routes = expert_route.reshape(-1)
    local_slot = flat_routes * capacity + slot_ranks(flat_routes, expert_total)
    share_width = width // lax.axis_size("tp")
    mid_share = lax.dynamic_slice_in_dim(mid, lax.axis_index("tp") * share_width, share_width, 1)
    buffer = (
        jnp.zeros((expert_total * capacity, width), jnp.bfloat16)
        .at[local_slot]
        .set(jnp.repeat(mid, top_count, 0))
    )
    arrived = lax.all_to_all(
        buffer.reshape(expert_total, capacity, width), "ep", split_axis=0, concat_axis=1, tiled=True
    )
    gate_pre = jnp.einsum("erd,edf->erf", arrived, w_expgate, preferred_element_type=jnp.float32)
    up_pre = jnp.einsum("erd,edf->erf", arrived, w_expup, preferred_element_type=jnp.float32)
    hidden_units = (jax.nn.silu(gate_pre) * up_pre).astype(jnp.bfloat16)
    down_terms = jnp.einsum(
        "erf,efd->erd", hidden_units, w_expdown, preferred_element_type=jnp.float32
    ).astype(jnp.bfloat16)
    expert_share = lax.psum_scatter(
        down_terms.astype(jnp.float32).astype(jnp.bfloat16), "tp", scatter_dimension=2, tiled=True
    )
    returned = lax.all_to_all(expert_share, "ep", split_axis=1, concat_axis=0, tiled=True)
    picked = returned.reshape(expert_total * capacity, share_width)[local_slot]
    picked = picked.astype(jnp.float32).reshape(own_rows, top_count, share_width)
    moe = first_weight[:, None] * picked[:, 0] + second_weight[:, None] * picked[:, 1]
    joined = res_alpha * mid_share.astype(jnp.float32) + moe
    row_sum, square_sum = lax.psum((jnp.sum(joined, -1), jnp.sum(joined * joined, -1)), "tp")
    row_mean = row_sum / D
    row_var = square_sum / D - row_mean * row_mean
    hidden_out = (
        (joined - row_mean[:, None]) * lax.rsqrt(row_var[:, None] + 1e-05) * second_gain
    ).astype(jnp.bfloat16)
    return (hidden_out, memory_next, new_max)


VMEM_LIMIT = 59 * 1024 * 1024


def announce(peers):
    barrier = pltpu.get_barrier_semaphore()
    for peer in peers:
        pl.semaphore_signal(barrier, inc=1, device_id=peer, device_id_type=MESH)
    return barrier


def remote(source, target, send_sem, recv_sem, peer):
    return pltpu.make_async_remote_copy(
        src_ref=source,
        dst_ref=target,
        send_sem=send_sem,
        recv_sem=recv_sem,
        device_id=peer,
        device_id_type=MESH,
    )


def flip(index, bits):
    result = index
    place = 1
    while place <= bits:
        if bits & place:
            result = result + place * (1 - 2 * lax.rem(lax.div(index, place), 2))
        place *= 2
    return result


def three_parts(value):
    high = value.astype(jnp.bfloat16).astype(jnp.float32)
    rest = value - high
    middle = rest.astype(jnp.bfloat16).astype(jnp.float32)
    return high, middle, rest - middle


def dot32(left, right):
    return jnp.dot(left, right, preferred_element_type=jnp.float32)


def dot_t(left, right):
    return lax.dot_general(left, right, (((1,), (1,)), ((), ())), preferred_element_type=jnp.float32)


def layer_kernel(
    n_ep,
    n_tp,
    groups,
    hidden_hbm,
    wq,
    wk,
    wv,
    wo,
    memory,
    w_out,
    w_gate,
    w_up,
    w_down,
    w_igate_t_hbm,
    w_fgate_t_hbm,
    input_bias_hbm,
    forget_bias_hbm,
    max_state_t_hbm,
    head_gain_hbm,
    gain1_hbm,
    gain2_hbm,
    group_router_t_hbm,
    expert_router_t_hbm,
    route_t_hbm,
    out_ref,
    mem_out,
    max_out,
    w_igate_t,
    w_fgate_t,
    input_bias,
    forget_bias,
    max_state_t,
    head_gain,
    gain1,
    gain2,
    group_router_t,
    expert_router_t,
    route_t,
    hid,
    weights,
    wo_buf,
    wg_buf,
    wu_buf,
    wd_buf,
    mem_half,
    gate_w,
    spread,
    proj_send,
    proj_recv,
    proj_own,
    far_own,
    far_recv,
    cross_send,
    cross_recv,
    cross_send2,
    cross_recv2,
    write_keys,
    keep_buf,
    value_buf,
    mix_send,
    mix_recv,
    sum_send,
    sum_recv,
    row_send,
    arrived,
    square_send,
    square_recv,
    stat_send,
    stat_recv,
    weight_buf,
    mid_buf,
    part_send,
    part_recv,
    wg_other,
    wu_other,
    wd_other,
    ret_send,
    ret_recv,
    stat2_send,
    stat2_recv,
    load_sem,
    small_sem,
    h_send,
    h_recv,
    p_send,
    p_recv,
    f_send,
    f_recv,
    c_send,
    c_recv,
    m_send,
    m_recv,
    u_send,
    u_recv,
    a_send,
    a_recv,
    b_send,
    b_recv,
    s_send,
    s_recv,
    d_send,
    d_recv,
    w_send,
    w_recv,
    r_send,
    r_recv,
    t_send,
    t_recv,
):
    me = lax.axis_index("ep")
    tp = lax.axis_index("tp")
    n_y = n_tp // 2
    y = lax.div(tp, 2)
    core = lax.rem(tp, 2)
    rows, width = hid.shape
    share = width // n_tp
    block = rows // groups
    heads = keep_buf.shape[0]
    depth, cols = wq.shape
    far_first = list(range(n_ep - 1, 0, -1))
    near_first = list(range(1, n_ep))
    ep_peer = [flip(me, k) for k in range(n_ep)]
    y_peer = [lax.rem(y + j, n_y) for j in range(n_y)]
    y_from = [lax.rem(y + n_y - j, n_y) for j in range(n_y)]
    tp_peer = [lax.rem(tp + o, n_tp) for o in range(n_tp)]
    partner = (me, 2 * y + 1 - core)

    def received(ref, sem):
        remote(ref, ref, sem, sem, partner).wait_recv()

    def sent(ref, sem):
        remote(ref, ref, sem, sem, partner).wait_send()

    def share_of(index):
        return pl.ds(pl.multiple_of(index * share, share), share)

    peers = [(ep_peer[k], tp) for k in range(1, n_ep)]
    peers += [(me, tp_peer[o]) for o in range(1, n_tp)]
    peers += [(ep_peer[k], 2 * y_peer[j] + core) for k in range(1, n_ep) for j in range(1, n_y)]
    barrier = announce(peers)
    hidden_load = pltpu.make_async_copy(hidden_hbm, hid, load_sem.at[0])
    hidden_load.start()
    small_loads = [
        pltpu.make_async_copy(source, target, small_sem.at[i])
        for i, (source, target) in enumerate(
            (
                (w_igate_t_hbm, w_igate_t),
                (w_fgate_t_hbm, w_fgate_t),
                (input_bias_hbm, input_bias),
                (forget_bias_hbm, forget_bias),
                (max_state_t_hbm, max_state_t),
                (head_gain_hbm, head_gain),
                (gain1_hbm, gain1),
                (gain2_hbm, gain2),
                (group_router_t_hbm, group_router_t),
                (expert_router_t_hbm, expert_router_t),
                (route_t_hbm, route_t),
            )
        )
    ]
    w_loads = [pltpu.make_async_copy(w, weights.at[i], load_sem.at[1]) for i, w in enumerate((wq, wk, wv, wo))]
    mem_load = pltpu.make_async_copy(memory, mem_out, load_sem.at[2])
    out_load = pltpu.make_async_copy(w_out, wo_buf, load_sem.at[3])
    gate_load = pltpu.make_async_copy(w_gate.at[0], wg_buf, load_sem.at[4])
    up_load = pltpu.make_async_copy(w_up.at[0], wu_buf, load_sem.at[5])
    down_load = pltpu.make_async_copy(w_down.at[0], wd_buf, load_sem.at[6])
    for load in small_loads + w_loads + [mem_load, out_load, gate_load, up_load, down_load]:
        load.start()
    hidden_load.wait()
    pl.semaphore_wait(barrier, len(peers))

    for k in far_first:
        columns = pl.ds(pl.multiple_of(ep_peer[k] * depth, depth), depth)
        remote(hid.at[:, columns], spread.at[k], h_send.at[0], h_recv.at[0], (ep_peer[k], tp)).start()
    spread[0] = hid[:, pl.ds(pl.multiple_of(me * depth, depth), depth)]
    for load in small_loads:
        load.wait()
    gate_w[...] = jnp.zeros_like(gate_w)
    in_rows = w_igate_t[...].astype(jnp.float32)
    forget_rows = w_fgate_t[...].astype(jnp.float32)
    for part in range(3):
        gate_w[2 * heads * part : 2 * heads * part + heads] = in_rows
        gate_w[2 * heads * part + heads : 2 * heads * (part + 1)] = forget_rows
    gate_half = gate_w[...].astype(jnp.bfloat16)

    mem_load.wait()

    def convert(b, carry):
        for h in range(heads):
            mem_half[h, pl.ds(pl.multiple_of(b * DH, DH), DH), :] = mem_out[b, pl.ds(h, DH, stride=heads), :].astype(
                jnp.bfloat16
            )
        return carry

    lax.fori_loop(0, rows, convert, 0)
    i_row = lax.broadcasted_iota(jnp.int32, (rows, rows), 0)
    i_col = lax.broadcasted_iota(jnp.int32, (rows, rows), 1)
    eye = i_row == i_col
    spread_row = lambda row: jnp.broadcast_to(row, (rows, rows))
    to_column = lambda row: jnp.sum(jnp.where(eye, spread_row(row), 0.0), 1, keepdims=True)
    to_row = lambda column: jnp.sum(jnp.where(eye, jnp.broadcast_to(column, (rows, rows)), 0.0), 0, keepdims=True)
    first_row = route_t[0:1, :].astype(jnp.float32)
    second_row = route_t[1:2, :].astype(jnp.float32)
    group_row = lax.shift_right_logical(route_t[0:1, :], GROUP_SIZE.bit_length() - 1).astype(jnp.float32)
    group_column = to_column(group_row)
    alike = jnp.broadcast_to(group_column, (rows, rows)) == spread_row(group_row)
    place_row = group_row * block + jnp.sum(jnp.where(alike & (i_row < i_col), 1.0, 0.0), 0, keepdims=True)
    place_column = to_column(place_row)
    perm_mask = spread_row(place_row) == i_row.astype(jnp.float32)
    perm = jnp.where(perm_mask, 1.0, 0.0).astype(jnp.bfloat16)
    back_mask = jnp.broadcast_to(place_column, (rows, rows)) == i_col.astype(jnp.float32)
    perm_back = jnp.where(back_mask, 1.0, 0.0).astype(jnp.bfloat16)
    first = jnp.sum(jnp.where(perm_mask, spread_row(first_row), 0.0), 1, keepdims=True)
    second = jnp.sum(jnp.where(perm_mask, spread_row(second_row), 0.0), 1, keepdims=True)
    hidden_sum = jnp.sum(dot32(perm, hid[...]), 1, keepdims=True)
    hidden_share = dot32(perm, hid[:, share_of(tp)])

    pltpu.make_async_copy(weights, weights, load_sem.at[1]).wait()
    received(spread.at[pl.ds(1, n_ep - 1)], h_recv.at[0])
    lhs = spread[...].reshape(n_ep * rows, depth)

    quad = GROUP_SIZE
    far_quads = range(1, n_ep // quad)
    bounds = [(0, cols), (cols, 2 * cols + DH), (2 * cols + DH, 3 * cols + DH), (3 * cols + DH, 4 * cols + DH)]
    cut = bounds[1][1]
    for i in range(4):
        part = dot32(lhs, weights[i])
        if i == 1:
            high, middle, low = three_parts(dot_t(lhs, gate_half))
            lane = lax.broadcasted_iota(jnp.int32, high.shape, 1)
            extra = jnp.where(lane < 2 * heads, high, jnp.where(lane < 4 * heads, middle, low))
            part = jnp.concatenate([part, extra], 1)
        span = slice(*bounds[i])
        proj_send[:, :, span] = part.astype(jnp.bfloat16).reshape(n_ep, rows, part.shape[1])
        proj_own[:, span] = part[:rows]
        for f in far_quads:
            far_own[f - 1, :, span] = part[f * quad * rows : (f * quad + 1) * rows]
        for f in far_quads:
            for j in range(quad - 1, 0, -1):
                remote(
                    proj_send.at[f * quad + j, :, span],
                    far_recv.at[f - 1, j - 1, :, span],
                    f_send.at[0],
                    f_recv.at[i],
                    (ep_peer[j], tp),
                ).start()
    for i in range(4):
        span = slice(*bounds[i])
        for j in range(quad - 1, 0, -1):
            remote(
                proj_send.at[j, :, span], proj_recv.at[j, :, span], p_send.at[0], p_recv.at[i], (ep_peer[j], tp)
            ).start()
    for i in range(4):
        span = slice(*bounds[i])
        received(far_recv.at[:, :, :, span], f_recv.at[i])
        for f in far_quads:
            summed = far_own[f - 1, :, span]
            for j in range(1, quad):
                summed += far_recv[f - 1, j - 1, :, span].astype(jnp.float32)
            if i < 2:
                source, target = cross_send.at[f - 1, :, span], cross_recv.at[f - 1, :, span]
                cross_send[f - 1, :, span] = summed
            else:
                span2 = slice(span.start - cut, span.stop - cut)
                source, target = cross_send2.at[f - 1, :, span2], cross_recv2.at[f - 1, :, span2]
                cross_send2[f - 1, :, span2] = summed.astype(jnp.bfloat16)
            remote(source, target, c_send.at[i // 2], c_recv.at[i], (ep_peer[f * quad], tp)).start()

    down_load.wait()
    gate_load.wait()
    up_load.wait()
    for j in range(n_y):
        place = share_of(2 * y_from[j] + 1 - core)
        remote(wg_buf.at[place], wg_other.at[j], w_send.at[0], w_recv.at[0], partner).start()
        remote(wu_buf.at[place], wu_other.at[j], w_send.at[1], w_recv.at[1], partner).start()
        theirs = wd_buf.at[:, share_of(2 * y_peer[j] + 1 - core)]
        remote(theirs, wd_other.at[j], w_send.at[2], w_recv.at[2], partner).start()

    def total(i):
        span = slice(*bounds[i])
        result = proj_own[:, span]
        received(proj_recv.at[pl.ds(1, quad - 1), :, span], p_recv.at[i])
        if i < 2:
            received(cross_recv.at[:, :, span], c_recv.at[i])
        else:
            received(cross_recv2.at[:, :, slice(span.start - cut, span.stop - cut)], c_recv.at[i])
        for j in range(1, quad):
            result += proj_recv[j, :, span].astype(jnp.float32)
        for f in far_quads:
            if i < 2:
                result += cross_recv[f - 1, :, span]
            else:
                result += cross_recv2[f - 1, :, span.start - cut : span.stop - cut].astype(jnp.float32)
        return result

    queries = total(0)
    read_old = []
    for h in range(heads):
        query = queries[:, h * DH : (h + 1) * DH]
        high = query.astype(jnp.bfloat16).astype(jnp.float32)
        both = jnp.concatenate([high, query - high], 0)
        row_of = lax.rem(lax.broadcasted_iota(jnp.int32, both.shape, 0), rows)
        spread_query = [jnp.where(row_of == b, both, 0.0).astype(jnp.bfloat16) for b in range(rows)]
        read = dot32(jnp.concatenate(spread_query, 1), mem_half[h])
        read_old.append(read[:rows] + read[rows:])
    second_total = total(1)
    keys = second_total[:, :cols] * DH ** (-0.5)
    gates = second_total[:, cols:]
    gates = gates + pltpu.roll(gates, DH - 2 * heads, 1) + pltpu.roll(gates, DH - 4 * heads, 1)
    scores = []
    for h in range(heads):
        span = slice(h * DH, (h + 1) * DH)
        scores.append(jnp.sum(queries[:, span] * keys[:, span], 1, keepdims=True))
    values = total(2)
    value_buf[...] = values
    last = total(3)
    mixed = []
    for h in range(heads):
        span = slice(h * DH, (h + 1) * DH)
        log_input = gates[:, h : h + 1] + input_bias[0:1, h : h + 1]
        forget = gates[:, heads + h : heads + h + 1] + forget_bias[0:1, h : h + 1]
        log_forget = jnp.minimum(forget, 0.0) - jnp.log1p(jnp.exp(-jnp.abs(forget)))
        carried = log_forget + to_column(max_state_t[h : h + 1, :])
        new_max = jnp.maximum(carried, log_input)
        keep = jnp.exp(carried - new_max)
        write = jnp.exp(log_input - new_max)
        max_out[h : h + 1, :] = to_row(new_max)
        keep_buf[h] = jnp.broadcast_to(keep, (rows, DH))
        write_keys[h * rows : (h + 1) * rows] = write * keys[:, span]
        readout = scores[h] * write * values[:, span] + keep * read_old[h]
        scaled = readout * lax.rsqrt(jnp.mean(readout * readout, -1, keepdims=True) + 1e-06)
        mixed.append((scaled * head_gain[:, span] * jax.nn.sigmoid(last[:, span])).astype(jnp.bfloat16))
    mixed_sorted = dot32(perm, jnp.concatenate(mixed, 1)).astype(jnp.bfloat16)

    out_load.wait()
    partial_sum = jnp.zeros((rows, 1), jnp.float32)
    order = [o for o in range(1, n_tp)] + [0]
    for o in order:
        part = dot32(mixed_sorted, wo_buf[:, share_of(tp_peer[o])]).astype(jnp.bfloat16)
        mix_send[o] = part
        partial_sum += jnp.sum(part.astype(jnp.float32), 1, keepdims=True)
        if o:
            remote(mix_send.at[o], mix_recv.at[o], m_send.at[0], m_recv.at[0], (me, tp_peer[o])).start()
    high, middle, low = three_parts(partial_sum)
    lane = lax.broadcasted_iota(jnp.int32, (rows, DH), 1)
    parts = jnp.where(lane == 0, high, jnp.where(lane == 1, middle, jnp.where(lane == 2, low, 0.0)))
    sum_send[...] = parts.astype(jnp.bfloat16)
    others = pl.ds(1, n_tp - 1)
    for o in range(1, n_tp):
        remote(sum_send, sum_recv.at[o], u_send.at[0], u_recv.at[0], (me, tp_peer[o])).start()
    joined = res_alpha * hidden_share + mix_send[0].astype(jnp.float32)
    row_sum = res_alpha * hidden_sum + partial_sum
    received(mix_recv.at[others], m_recv.at[0])
    received(sum_recv.at[others], u_recv.at[0])
    for o in range(1, n_tp):
        joined += mix_recv[o].astype(jnp.float32)
        row_sum += jnp.sum(sum_recv[o].astype(jnp.float32), 1, keepdims=True)
    centred = joined - row_sum / width
    scaled_rows = centred * gain1[:, share_of(tp)]
    for g in range(groups):
        row_send[g] = scaled_rows[g * block : (g + 1) * block].astype(jnp.bfloat16)
    for k in far_first + [0]:
        for j in range(n_y - 1, -1, -1):
            if k or j:
                remote(
                    row_send.at[lax.div(ep_peer[k], GROUP_SIZE)],
                    arrived.at[j, k],
                    a_send.at[min(j, 1)],
                    a_recv.at[k],
                    (ep_peer[k], 2 * y_peer[j] + core),
                ).start()
    arrived[0, 0] = row_send[lax.div(me, GROUP_SIZE)]

    experts = expert_router_t.shape[0]
    expert_part = jnp.zeros((rows, experts), jnp.float32)
    group_part = jnp.zeros((rows, groups), jnp.float32)
    for piece in three_parts(scaled_rows):
        half = piece.astype(jnp.bfloat16)
        expert_part += dot_t(half, expert_router_t[:, share_of(tp)])
        group_part += dot_t(half, group_router_t[:, share_of(tp)])
    stat_send[...] = jnp.zeros_like(stat_send)
    stat_send[:, 0:experts] = expert_part
    stat_send[:, experts : experts + groups] = group_part
    stat_send[:, experts + groups : experts + groups + 1] = jnp.sum(centred * centred, 1, keepdims=True)
    for o in range(1, n_tp):
        remote(stat_send, stat_recv.at[o], s_send.at[0], s_recv.at[0], (me, tp_peer[o])).start()

    keys_t = write_keys[...].T
    for b in range(rows):
        for h in range(heads):
            old = mem_out[b, pl.ds(h, DH, stride=heads), :]
            column = keys_t[:, h * rows + b : h * rows + b + 1]
            value = value_buf[b : b + 1, h * DH : (h + 1) * DH]
            mem_out[b, pl.ds(h, DH, stride=heads), :] = keep_buf[h, b : b + 1, :] * old + column * value

    stat_total = stat_send[...]
    received(stat_recv.at[others], s_recv.at[0])
    for o in range(1, n_tp):
        stat_total += stat_recv[o]
    row_scale = lax.rsqrt(stat_total[:, experts + groups : experts + groups + 1] / width + 1e-05)
    logits = stat_total * row_scale
    lanes = lax.broadcasted_iota(jnp.int32, logits.shape, 1).astype(jnp.float32)
    pick = lambda index: jnp.sum(jnp.where(lanes == index, logits, 0.0), 1, keepdims=True)
    first_logit = pick(first)
    second_logit = pick(second)
    group_gate = jax.nn.sigmoid(pick(experts + jnp.floor(first / GROUP_SIZE)))
    weight1 = group_gate * jax.nn.sigmoid(first_logit - second_logit)
    weight2 = group_gate * jax.nn.sigmoid(second_logit - first_logit)
    mid = (scaled_rows * row_scale).astype(jnp.bfloat16).astype(jnp.float32)
    for g in range(groups):
        span = slice(g * block, (g + 1) * block)
        for slot, column in enumerate((first, second, weight1, weight2)):
            weight_buf[slot, g] = jnp.broadcast_to(column[span], (block, DH))
        mid_buf[g] = res_alpha * mid[span]

    received(wg_other, w_recv.at[0])
    received(wu_other, w_recv.at[1])
    received(wd_other, w_recv.at[2])
    for k in [0] + near_first:
        first_j = 0 if k else 1
        received(arrived.at[pl.ds(first_j, n_y - first_j), k], a_recv.at[k])
    count = n_ep * block
    hidden_units = wg_buf.shape[1]
    tokens32 = [arrived[j].astype(jnp.float32).reshape(count, share) for j in range(n_y)]
    tokens = [token.astype(jnp.bfloat16) for token in tokens32]
    places = [share_of(2 * y_from[j] + core) for j in range(n_y)]
    squares = jnp.zeros((count, DH), jnp.float32)
    for j in range(n_y):
        plain = tokens32[j] / gain1[:, places[j]]
        plain = plain * plain
        for c in range(share // DH):
            squares += plain[:, c * DH : (c + 1) * DH]
    square_send[...] = squares
    remote(square_send, square_recv, b_send.at[0], b_recv.at[0], partner).start()
    partial = []
    for side in range(2):
        gate_pre = jnp.zeros((count, hidden_units), jnp.float32)
        up_pre = jnp.zeros((count, hidden_units), jnp.float32)
        for j in range(n_y):
            gate_pre += dot32(tokens[j], wg_other[j] if side else wg_buf[places[j], :])
            up_pre += dot32(tokens[j], wu_other[j] if side else wu_buf[places[j], :])
        partial.append((gate_pre, up_pre))
        part_send[side, :, 0:hidden_units] = gate_pre.astype(jnp.bfloat16)
        part_send[side, :, hidden_units:] = up_pre.astype(jnp.bfloat16)
        remote(part_send.at[side], part_recv.at[side], d_send.at[0], d_recv.at[0], partner).start()
    received(square_recv, b_recv.at[0])
    squares += square_recv[...]
    token_scale = lax.rsqrt(jnp.sum(squares, 1, keepdims=True) / width + 1e-05)
    received(part_recv, d_recv.at[0])
    units = []
    for side in range(2):
        gate_pre = (partial[side][0] + part_recv[1 - side, :, 0:hidden_units].astype(jnp.float32)) * token_scale
        up_pre = (partial[side][1] + part_recv[1 - side, :, hidden_units:].astype(jnp.float32)) * token_scale
        units.append((gate_pre * jax.nn.sigmoid(gate_pre) * up_pre).astype(jnp.bfloat16))

    for j in range(n_y - 1, -1, -1):
        result = dot32(units[0], wd_buf[:, share_of(2 * y_peer[j] + core)]) + dot32(units[1], wd_other[j])
        for k in range(n_ep):
            ret_send[j, k] = result[k * block : (k + 1) * block].astype(jnp.bfloat16)
    for k in far_first + [0]:
        for j in range(n_y - 1, -1, -1):
            if k or j:
                remote(
                    ret_send.at[j, k],
                    ret_recv.at[j, k],
                    r_send.at[min(j, 1)],
                    r_recv.at[k],
                    (ep_peer[k], 2 * y_peer[j] + core),
                ).start()
    for piece in range(groups):
        g = flip(lax.div(me, GROUP_SIZE), piece)
        gathered = mid_buf[g]
        for k in range(piece * GROUP_SIZE, (piece + 1) * GROUP_SIZE):
            expert = ep_peer[k].astype(jnp.float32)
            weight = jnp.where(weight_buf[0, g] == expert, weight_buf[2, g], 0.0)
            weight += jnp.where(weight_buf[1, g] == expert, weight_buf[3, g], 0.0)
            first_j = 0 if k else 1
            received(ret_recv.at[pl.ds(first_j, n_y - first_j), k], r_recv.at[k])
            result = jnp.zeros((block, share), jnp.float32)
            for j in range(n_y):
                result += (ret_recv[j, k] if k or j else ret_send[0, 0]).astype(jnp.float32)
            gathered += weight[:, 0:1] * result
        mid_buf[g] = gathered
    joined = mid_buf[...].reshape(rows, share)
    row_sum = jnp.sum(joined, -1, keepdims=True)
    square_sum = jnp.sum(joined * joined, -1, keepdims=True)
    stat2_send[...] = jnp.where(lane == 0, row_sum, square_sum)
    for o in range(1, n_tp):
        remote(stat2_send, stat2_recv.at[o], t_send.at[0], t_recv.at[0], (me, tp_peer[o])).start()
    received(stat2_recv.at[others], t_recv.at[0])
    for o in range(1, n_tp):
        row_sum += stat2_recv[o][:, 0:1]
        square_sum += stat2_recv[o][:, 1:2]
    row_mean = row_sum / width
    row_var = square_sum / width - row_mean * row_mean
    result = ((joined - row_mean) * lax.rsqrt(row_var + 1e-05) * gain2[...]).astype(jnp.bfloat16)
    out_ref[...] = dot32(perm_back, result).astype(jnp.bfloat16)
    rest = pl.ds(1, n_ep - 1)
    for ref, sem in (
        (spread.at[rest], h_send.at[0]),
        (far_recv, f_send.at[0]),
        (proj_recv.at[pl.ds(1, quad - 1)], p_send.at[0]),
        (cross_send, c_send.at[0]),
        (cross_send2, c_send.at[1]),
        (mix_send.at[others], m_send.at[0]),
        (sum_recv.at[others], u_send.at[0]),
        (arrived.at[0, rest], a_send.at[0]),
        (arrived.at[pl.ds(1, n_y - 1)], a_send.at[1]),
        (stat_recv.at[others], s_send.at[0]),
        (square_send, b_send.at[0]),
        (part_send, d_send.at[0]),
        (wg_other, w_send.at[0]),
        (wu_other, w_send.at[1]),
        (wd_other, w_send.at[2]),
        (ret_send.at[0, rest], r_send.at[0]),
        (ret_send.at[pl.ds(1, n_y - 1)], r_send.at[1]),
        (stat2_recv.at[others], t_send.at[0]),
    ):
        sent(ref, sem)


def layer(n_ep, n_tp, groups, *operands):
    hidden, wq, _, _, _, memory, w_out, w_gate, _, w_down = operands[:10]
    rows, width = hidden.shape
    heads = memory.shape[1] // DH
    depth, cols = wq.shape
    share = width // n_tp
    block = rows // groups
    n_y = n_tp // 2
    half, full = jnp.bfloat16, jnp.float32
    vmem = pl.BlockSpec(memory_space=pltpu.VMEM)
    anywhere = pl.BlockSpec(memory_space=pl.ANY)
    dma = pltpu.SemaphoreType.DMA
    count = n_ep * block
    wide = 4 * cols + DH
    n_far = n_ep // GROUP_SIZE - 1
    return pl.pallas_call(
        functools.partial(layer_kernel, n_ep, n_tp, groups),
        out_shape=(
            pltpu.VMEM((rows, share), half),
            pltpu.VMEM(memory.shape, full),
            pltpu.VMEM((heads, rows), full),
        ),
        in_specs=[anywhere] * len(operands),
        out_specs=(vmem, vmem, vmem),
        scratch_shapes=[pltpu.VMEM(x.shape, x.dtype) for x in operands[10:]]
        + [
            pltpu.VMEM((rows, width), half),
            pltpu.VMEM((4, depth, cols), half),
            pltpu.VMEM(w_out.shape, half),
            pltpu.VMEM(w_gate.shape[1:], half),
            pltpu.VMEM(w_gate.shape[1:], half),
            pltpu.VMEM(w_down.shape[1:], half),
            pltpu.VMEM((heads, rows * DH, DH), half),
            pltpu.VMEM((DH, depth), full),
            pltpu.VMEM((n_ep, rows, depth), half),
            pltpu.VMEM((n_ep, rows, wide), half),
            pltpu.VMEM((n_ep, rows, wide), half),
            pltpu.VMEM((rows, wide), full),
            pltpu.VMEM((n_far, rows, wide), full),
            pltpu.VMEM((n_far, GROUP_SIZE - 1, rows, wide), half),
            pltpu.VMEM((n_far, rows, 2 * cols + DH), full),
            pltpu.VMEM((n_far, rows, 2 * cols + DH), full),
            pltpu.VMEM((n_far, rows, 2 * cols), half),
            pltpu.VMEM((n_far, rows, 2 * cols), half),
            pltpu.VMEM((heads * rows, DH), full),
            pltpu.VMEM((heads, rows, DH), full),
            pltpu.VMEM((rows, cols), full),
            pltpu.VMEM((n_tp, rows, share), half),
            pltpu.VMEM((n_tp, rows, share), half),
            pltpu.VMEM((rows, DH), half),
            pltpu.VMEM((n_tp, rows, DH), half),
            pltpu.VMEM((groups, block, share), half),
            pltpu.VMEM((n_y, n_ep, block, share), half),
            pltpu.VMEM((count, DH), full),
            pltpu.VMEM((count, DH), full),
            pltpu.VMEM((rows, DH), full),
            pltpu.VMEM((n_tp, rows, DH), full),
            pltpu.VMEM((4, groups, block, DH), full),
            pltpu.VMEM((groups, block, share), full),
            pltpu.VMEM((2, count, 2 * w_gate.shape[2]), half),
            pltpu.VMEM((2, count, 2 * w_gate.shape[2]), half),
            pltpu.VMEM((n_y, share, w_gate.shape[2]), half),
            pltpu.VMEM((n_y, share, w_gate.shape[2]), half),
            pltpu.VMEM((n_y, w_down.shape[1], share), half),
            pltpu.VMEM((n_y, n_ep, block, share), half),
            pltpu.VMEM((n_y, n_ep, block, share), half),
            pltpu.VMEM((rows, DH), full),
            pltpu.VMEM((n_tp, rows, DH), full),
            dma((7,)),
            dma((len(operands) - 10,)),
            dma((1,)),
            dma((1,)),
            dma((1,)),
            dma((4,)),
            dma((1,)),
            dma((4,)),
            dma((2,)),
            dma((4,)),
            dma((1,)),
            dma((1,)),
            dma((1,)),
            dma((1,)),
            dma((2,)),
            dma((n_ep,)),
            dma((1,)),
            dma((1,)),
            dma((1,)),
            dma((1,)),
            dma((1,)),
            dma((1,)),
            dma((3,)),
            dma((3,)),
            dma((2,)),
            dma((n_ep,)),
            dma((1,)),
            dma((1,)),
        ],
        compiler_params=pltpu.CompilerParams(
            collective_id=0, has_side_effects=True, vmem_limit_bytes=VMEM_LIMIT
        ),
        name="layer",
    )(*operands)


def store_kernel(result, memory, new_max, out_ref, mem_out, max_out, sems):
    copies = [
        pltpu.make_async_copy(source, target, sems.at[i])
        for i, (source, target) in enumerate(((memory, mem_out), (result, out_ref), (new_max, max_out)))
    ]
    for copy in copies:
        copy.start()
    for copy in copies:
        copy.wait()


def store(*operands):
    anywhere = pl.BlockSpec(memory_space=pl.ANY)
    return pl.pallas_call(
        store_kernel,
        out_shape=tuple(jax.ShapeDtypeStruct(x.shape, x.dtype) for x in operands),
        in_specs=[anywhere] * 3,
        out_specs=(anywhere,) * 3,
        scratch_shapes=[pltpu.SemaphoreType.DMA((3,))],
        compiler_params=pltpu.CompilerParams(vmem_limit_bytes=1 << 20),
        name="store",
    )(*operands)


def kernel_body(
    hidden_in,
    w_query,
    w_key,
    w_value,
    w_outgate,
    w_igate,
    w_fgate,
    input_bias,
    forget_bias,
    mem_state,
    max_state,
    head_gain,
    w_output,
    first_gain,
    w_group_router,
    w_expert_router,
    expert_route,
    w_expgate,
    w_expup,
    w_expdown,
    second_gain,
):
    n_ep, n_tp = lax.axis_size("ep"), lax.axis_size("tp")
    rows, heads, flat = mem_state.shape
    groups = w_group_router.shape[1]
    memory = mem_state.reshape(rows, heads, DH, DH).transpose(0, 2, 1, 3).reshape(rows, DH * heads, DH)
    results = layer(
        n_ep,
        n_tp,
        groups,
        hidden_in,
        w_query,
        w_key,
        w_value,
        w_outgate,
        memory,
        w_output,
        w_expgate,
        w_expup,
        w_expdown,
        w_igate.T,
        w_fgate.T,
        input_bias[None],
        forget_bias[None],
        max_state.T,
        head_gain[None],
        first_gain[None],
        second_gain[None],
        w_group_router.T,
        w_expert_router.T,
        expert_route.T,
    )
    hidden_out, memory_next, max_next = store(*results)
    memory_next = memory_next.reshape(rows, DH, heads, DH).transpose(0, 2, 1, 3).reshape(rows, heads, flat)
    return (hidden_out, memory_next, max_next.T)


def either_body(*operands):
    hidden_in, w_query, group_router, experts = operands[0], operands[1], operands[14], operands[17]
    rows, width = hidden_in.shape
    n_ep, n_tp = lax.axis_size("ep"), lax.axis_size("tp")
    groups = group_router.shape[1]
    block, odd_rows = divmod(rows, groups)
    aligned = rows % 16 == 0 and block % 8 == 0 and odd_rows == 0 and experts.shape[0] == 1
    aligned = aligned and w_query.shape[0] % DH == 0 and width // n_tp % DH == 0
    aligned = aligned and n_tp % 2 == 0 and n_ep & (n_ep - 1) == 0 and n_ep == groups * GROUP_SIZE and groups > 1
    return (kernel_body if aligned else body)(*operands)


def solution(mesh):
    return jax.shard_map(
        either_body,
        mesh=mesh,
        in_specs=(
            P("ep", None),
            P("ep", "tp"),
            P("ep", "tp"),
            P("ep", "tp"),
            P("ep", "tp"),
            P("ep", "tp"),
            P("ep", "tp"),
            P("tp"),
            P("tp"),
            P("ep", "tp", None),
            P("ep", "tp"),
            P("tp"),
            P("tp", None),
            P(),
            P(),
            P(),
            P("ep", None),
            P("ep", None, "tp"),
            P("ep", None, "tp"),
            P("ep", "tp", None),
            P("tp"),
        ),
        out_specs=(P("ep", "tp"), P("ep", "tp", None), P("ep", "tp")),
        check_vma=False,
    )
```

```python
import functools

import jax
import jax.numpy as jnp
from jax import lax
from jax.experimental import pallas as pl
from jax.experimental.pallas import tpu as pltpu
from jax.sharding import PartitionSpec as P

D = 4096
DH = 128
GROUP_SIZE = 4
MESH = pl.DeviceIdType.MESH


res_alpha = 8.0**0.25


def layer_norm(values, gain):
    row_mean = jnp.mean(values, -1, keepdims=True)
    row_var = jnp.mean(values * values, -1, keepdims=True) - row_mean * row_mean
    return (values - row_mean) * lax.rsqrt(row_var + 1e-05) * gain


def mlstm_step(queries, keys_scaled, values, log_input, log_forget, memory, stabilizer):
    new_max = jnp.maximum(log_forget + stabilizer, log_input)
    keep_old = jnp.exp(log_forget + stabilizer - new_max)
    write_new = jnp.exp(log_input - new_max)
    scores = jnp.sum(queries * keys_scaled, -1) * write_new
    read_old = jnp.einsum("bhd,bhde->bhe", queries, memory, precision=lax.Precision.HIGHEST)
    readout = scores[..., None] * values + keep_old[..., None] * read_old
    memory_next = (
        keep_old[..., None, None] * memory
        + write_new[..., None, None] * keys_scaled[..., :, None] * values[..., None, :]
    )
    return (readout, memory_next, new_max)


def head_mix(readout, head_gain, out_pre):
    scaled = readout * lax.rsqrt(jnp.mean(readout * readout, -1, keepdims=True) + 1e-06)
    flat_heads = scaled.reshape(scaled.shape[0], -1)
    return (flat_heads * head_gain * jax.nn.sigmoid(out_pre)).astype(jnp.bfloat16)


def route_weights(mid_float, w_group_router, w_expert_router, expert_route):
    group_logits = jnp.dot(
        mid_float, w_group_router.astype(jnp.float32), precision=lax.Precision.HIGHEST
    )
    expert_logits = jnp.dot(
        mid_float, w_expert_router.astype(jnp.float32), precision=lax.Precision.HIGHEST
    )
    first_expert = expert_route[:, 0]
    second_expert = expert_route[:, 1]
    expert_ids = lax.broadcasted_iota(jnp.int32, expert_logits.shape, 1)
    group_ids = lax.broadcasted_iota(jnp.int32, group_logits.shape, 1)
    first_logit = jnp.sum(jnp.where(expert_ids == first_expert[:, None], expert_logits, 0.0), -1)
    second_logit = jnp.sum(jnp.where(expert_ids == second_expert[:, None], expert_logits, 0.0), -1)
    group_pick = jnp.sum(
        jnp.where(group_ids == (first_expert // GROUP_SIZE)[:, None], group_logits, 0.0), -1
    )
    group_gate = jax.nn.sigmoid(group_pick)
    return (
        group_gate * jax.nn.sigmoid(first_logit - second_logit),
        group_gate * jax.nn.sigmoid(second_logit - first_logit),
    )


def slot_ranks(flat_routes, expert_total):
    onehot = (
        flat_routes[:, None]
        == lax.broadcasted_iota(jnp.int32, (flat_routes.shape[0], expert_total), 1)
    ).astype(jnp.int32)
    running = jnp.cumsum(onehot, 0)
    return jnp.sum((running - 1) * onehot, -1)


def body(
    hidden_in,
    w_query,
    w_key,
    w_value,
    w_outgate,
    w_igate,
    w_fgate,
    input_bias,
    forget_bias,
    mem_state,
    max_state,
    head_gain,
    w_output,
    first_gain,
    w_group_router,
    w_expert_router,
    expert_route,
    w_expgate,
    w_expup,
    w_expdown,
    second_gain,
):
    own_rows, width = hidden_in.shape
    heads_here = mem_state.shape[1]
    head_width = heads_here * DH
    top_count = expert_route.shape[1]
    spread_rows = lax.all_to_all(hidden_in, "ep", split_axis=1, concat_axis=0, tiled=True)
    stacked_w = jnp.concatenate([w_query, w_key, w_value, w_outgate], 1)
    gate_w = jnp.concatenate([w_igate, w_fgate], 1)
    proj_terms = jnp.dot(spread_rows, stacked_w, preferred_element_type=jnp.float32)
    gate_terms = jnp.dot(spread_rows, gate_w, preferred_element_type=jnp.float32)
    projected, gate_sums = (
        lax.psum_scatter(proj_terms, "ep", scatter_dimension=0, tiled=True),
        lax.psum_scatter(gate_terms, "ep", scatter_dimension=0, tiled=True),
    )
    shaped = projected.reshape(own_rows, 4, heads_here, DH)
    queries = shaped[:, 0]
    keys_raw = shaped[:, 1]
    values = shaped[:, 2]
    out_pre = shaped[:, 3].reshape(own_rows, head_width)
    input_sum = gate_sums[:, :heads_here]
    forget_sum = gate_sums[:, heads_here:]
    keys_scaled = keys_raw * DH ** (-0.5)
    log_input = input_sum + input_bias
    log_forget = jax.nn.log_sigmoid(forget_sum + forget_bias)
    memory = mem_state.reshape(own_rows, heads_here, DH, DH)
    readout, memory_square, new_max = mlstm_step(
        queries, keys_scaled, values, log_input, log_forget, memory, max_state
    )
    memory_next = memory_square.reshape(own_rows, heads_here, DH * DH)
    mixed_heads = head_mix(readout, head_gain, out_pre)
    partial_mix = jnp.dot(mixed_heads, w_output, preferred_element_type=jnp.float32).astype(
        jnp.bfloat16
    )
    mix = lax.psum(partial_mix.astype(jnp.float32).astype(jnp.bfloat16), "tp").astype(jnp.float32)
    mid_float = layer_norm(res_alpha * hidden_in.astype(jnp.float32) + mix, first_gain)
    mid = mid_float.astype(jnp.bfloat16)
    first_weight, second_weight = route_weights(
        mid_float, w_group_router, w_expert_router, expert_route
    )
    expert_total = w_expgate.shape[0] * lax.axis_size("ep")
    capacity = 2 * own_rows * top_count // expert_total
    flat_routes = expert_route.reshape(-1)
    local_slot = flat_routes * capacity + slot_ranks(flat_routes, expert_total)
    share_width = width // lax.axis_size("tp")
    mid_share = lax.dynamic_slice_in_dim(mid, lax.axis_index("tp") * share_width, share_width, 1)
    buffer = (
        jnp.zeros((expert_total * capacity, width), jnp.bfloat16)
        .at[local_slot]
        .set(jnp.repeat(mid, top_count, 0))
    )
    arrived = lax.all_to_all(
        buffer.reshape(expert_total, capacity, width), "ep", split_axis=0, concat_axis=1, tiled=True
    )
    gate_pre = jnp.einsum("erd,edf->erf", arrived, w_expgate, preferred_element_type=jnp.float32)
    up_pre = jnp.einsum("erd,edf->erf", arrived, w_expup, preferred_element_type=jnp.float32)
    hidden_units = (jax.nn.silu(gate_pre) * up_pre).astype(jnp.bfloat16)
    down_terms = jnp.einsum(
        "erf,efd->erd", hidden_units, w_expdown, preferred_element_type=jnp.float32
    ).astype(jnp.bfloat16)
    expert_share = lax.psum_scatter(
        down_terms.astype(jnp.float32).astype(jnp.bfloat16), "tp", scatter_dimension=2, tiled=True
    )
    returned = lax.all_to_all(expert_share, "ep", split_axis=1, concat_axis=0, tiled=True)
    picked = returned.reshape(expert_total * capacity, share_width)[local_slot]
    picked = picked.astype(jnp.float32).reshape(own_rows, top_count, share_width)
    moe = first_weight[:, None] * picked[:, 0] + second_weight[:, None] * picked[:, 1]
    joined = res_alpha * mid_share.astype(jnp.float32) + moe
    row_sum, square_sum = lax.psum((jnp.sum(joined, -1), jnp.sum(joined * joined, -1)), "tp")
    row_mean = row_sum / D
    row_var = square_sum / D - row_mean * row_mean
    hidden_out = (
        (joined - row_mean[:, None]) * lax.rsqrt(row_var[:, None] + 1e-05) * second_gain
    ).astype(jnp.bfloat16)
    return (hidden_out, memory_next, new_max)


VMEM_LIMIT = 59 * 1024 * 1024


def announce(peers):
    barrier = pltpu.get_barrier_semaphore()
    for peer in peers:
        pl.semaphore_signal(barrier, inc=1, device_id=peer, device_id_type=MESH)
    return barrier


def remote(source, target, send_sem, recv_sem, peer):
    return pltpu.make_async_remote_copy(
        src_ref=source,
        dst_ref=target,
        send_sem=send_sem,
        recv_sem=recv_sem,
        device_id=peer,
        device_id_type=MESH,
    )


def flip(index, bits):
    result = index
    place = 1
    while place <= bits:
        if bits & place:
            result = result + place * (1 - 2 * lax.rem(lax.div(index, place), 2))
        place *= 2
    return result


def three_parts(value):
    high = value.astype(jnp.bfloat16).astype(jnp.float32)
    rest = value - high
    middle = rest.astype(jnp.bfloat16).astype(jnp.float32)
    return high, middle, rest - middle


def dot32(left, right):
    return jnp.dot(left, right, preferred_element_type=jnp.float32)


def dot_t(left, right):
    return lax.dot_general(left, right, (((1,), (1,)), ((), ())), preferred_element_type=jnp.float32)


def layer_kernel(
    n_ep,
    n_tp,
    groups,
    hidden_hbm,
    wq,
    wk,
    wv,
    wo,
    memory,
    w_out,
    w_gate,
    w_up,
    w_down,
    w_igate_t_hbm,
    w_fgate_t_hbm,
    input_bias_hbm,
    forget_bias_hbm,
    max_state_t_hbm,
    head_gain_hbm,
    gain1_hbm,
    gain2_hbm,
    group_router_t_hbm,
    expert_router_t_hbm,
    route_t_hbm,
    out_ref,
    mem_out,
    max_out,
    w_igate_t,
    w_fgate_t,
    input_bias,
    forget_bias,
    max_state_t,
    head_gain,
    gain1,
    gain2,
    group_router_t,
    expert_router_t,
    route_t,
    hid,
    weights,
    wo_buf,
    wg_buf,
    wu_buf,
    wd_buf,
    mem_half,
    gate_w,
    spread,
    proj_send,
    proj_recv,
    proj_own,
    far_own,
    far_recv,
    cross_send,
    cross_recv,
    cross_send2,
    cross_recv2,
    write_keys,
    keep_buf,
    value_buf,
    mix_send,
    mix_recv,
    sum_send,
    sum_recv,
    row_send,
    arrived,
    square_send,
    square_recv,
    stat_send,
    stat_recv,
    weight_buf,
    mid_buf,
    part_send,
    part_recv,
    wg_other,
    wu_other,
    wd_other,
    ret_send,
    ret_recv,
    stat2_send,
    stat2_recv,
    load_sem,
    h_send,
    h_recv,
    p_send,
    p_recv,
    f_send,
    f_recv,
    c_send,
    c_recv,
    m_send,
    m_recv,
    u_send,
    u_recv,
    a_send,
    a_recv,
    b_send,
    b_recv,
    s_send,
    s_recv,
    d_send,
    d_recv,
    w_send,
    w_recv,
    r_send,
    r_recv,
    t_send,
    t_recv,
):
    me = lax.axis_index("ep")
    tp = lax.axis_index("tp")
    n_y = n_tp // 2
    y = lax.div(tp, 2)
    core = lax.rem(tp, 2)
    rows, width = hid.shape
    share = width // n_tp
    block = rows // groups
    heads = keep_buf.shape[0]
    depth, cols = wq.shape
    far_first = list(range(n_ep - 1, 0, -1))
    near_first = list(range(1, n_ep))
    ep_peer = [flip(me, k) for k in range(n_ep)]
    y_peer = [lax.rem(y + j, n_y) for j in range(n_y)]
    y_from = [lax.rem(y + n_y - j, n_y) for j in range(n_y)]
    tp_peer = [flip(tp, o) for o in range(n_tp)]
    partner = (me, 2 * y + 1 - core)

    def received(ref, sem):
        remote(ref, ref, sem, sem, partner).wait_recv()

    def sent(ref, sem):
        remote(ref, ref, sem, sem, partner).wait_send()

    def share_of(index):
        return pl.ds(pl.multiple_of(index * share, share), share)

    peers = [(ep_peer[k], tp) for k in range(1, n_ep)]
    peers += [(me, tp_peer[o]) for o in range(1, n_tp)]
    peers += [(ep_peer[k], 2 * y_peer[j] + core) for k in range(1, n_ep) for j in range(1, n_y)]
    barrier = announce(peers)
    hidden_load = pltpu.make_async_copy(hidden_hbm, hid, load_sem.at[0])
    hidden_load.start()
    small_loads = [
        pltpu.make_async_copy(source, target, sem)
        for sem, (source, target) in zip(
            (p_send.at[0], f_send.at[0], c_send.at[0], c_send.at[1], m_send.at[0], u_send.at[0], a_send.at[0], a_send.at[1], b_send.at[0], s_send.at[0], d_send.at[0]),
            (
                (w_igate_t_hbm, w_igate_t),
                (w_fgate_t_hbm, w_fgate_t),
                (input_bias_hbm, input_bias),
                (forget_bias_hbm, forget_bias),
                (max_state_t_hbm, max_state_t),
                (head_gain_hbm, head_gain),
                (gain1_hbm, gain1),
                (gain2_hbm, gain2),
                (group_router_t_hbm, group_router_t),
                (expert_router_t_hbm, expert_router_t),
                (route_t_hbm, route_t),
            )
        )
    ]
    w_loads = [pltpu.make_async_copy(w, weights.at[i], load_sem.at[1]) for i, w in enumerate((wq, wk, wv, wo))]
    mem_load = pltpu.make_async_copy(memory, mem_out, load_sem.at[2])
    out_load = pltpu.make_async_copy(w_out, wo_buf, load_sem.at[3])
    gate_load = pltpu.make_async_copy(w_gate.at[0], wg_buf, load_sem.at[4])
    up_load = pltpu.make_async_copy(w_up.at[0], wu_buf, load_sem.at[5])
    down_load = pltpu.make_async_copy(w_down.at[0], wd_buf, load_sem.at[6])
    for load in small_loads + w_loads + [mem_load, out_load, gate_load, up_load, down_load]:
        load.start()
    hidden_load.wait()
    pl.semaphore_wait(barrier, len(peers))

    for k in far_first:
        columns = pl.ds(pl.multiple_of(ep_peer[k] * depth, depth), depth)
        remote(hid.at[:, columns], spread.at[k], h_send.at[0], h_recv.at[0], (ep_peer[k], tp)).start()
    spread[0] = hid[:, pl.ds(pl.multiple_of(me * depth, depth), depth)]
    for load in small_loads:
        load.wait()
    gate_w[...] = jnp.zeros_like(gate_w)
    in_rows = w_igate_t[...].astype(jnp.float32)
    forget_rows = w_fgate_t[...].astype(jnp.float32)
    for part in range(3):
        gate_w[2 * heads * part : 2 * heads * part + heads] = in_rows
        gate_w[2 * heads * part + heads : 2 * heads * (part + 1)] = forget_rows
    gate_half = gate_w[...].astype(jnp.bfloat16)

    mem_load.wait()

    def convert(b, carry):
        for h in range(heads):
            mem_half[h, pl.ds(pl.multiple_of(b * DH, DH), DH), :] = mem_out[b, pl.ds(h, DH, stride=heads), :].astype(
                jnp.bfloat16
            )
        return carry

    lax.fori_loop(0, rows, convert, 0)
    i_row = lax.broadcasted_iota(jnp.int32, (rows, rows), 0)
    i_col = lax.broadcasted_iota(jnp.int32, (rows, rows), 1)
    eye = i_row == i_col
    spread_row = lambda row: jnp.broadcast_to(row, (rows, rows))
    to_column = lambda row: jnp.sum(jnp.where(eye, spread_row(row), 0.0), 1, keepdims=True)
    to_row = lambda column: jnp.sum(jnp.where(eye, jnp.broadcast_to(column, (rows, rows)), 0.0), 0, keepdims=True)
    first_row = route_t[0:1, :].astype(jnp.float32)
    second_row = route_t[1:2, :].astype(jnp.float32)
    group_row = lax.shift_right_logical(route_t[0:1, :], GROUP_SIZE.bit_length() - 1).astype(jnp.float32)
    group_column = to_column(group_row)
    alike = jnp.broadcast_to(group_column, (rows, rows)) == spread_row(group_row)
    place_row = group_row * block + jnp.sum(jnp.where(alike & (i_row < i_col), 1.0, 0.0), 0, keepdims=True)
    place_column = to_column(place_row)
    perm_mask = spread_row(place_row) == i_row.astype(jnp.float32)
    perm = jnp.where(perm_mask, 1.0, 0.0).astype(jnp.bfloat16)
    back_mask = jnp.broadcast_to(place_column, (rows, rows)) == i_col.astype(jnp.float32)
    perm_back = jnp.where(back_mask, 1.0, 0.0).astype(jnp.bfloat16)
    first = jnp.sum(jnp.where(perm_mask, spread_row(first_row), 0.0), 1, keepdims=True)
    second = jnp.sum(jnp.where(perm_mask, spread_row(second_row), 0.0), 1, keepdims=True)
    hidden_sum = jnp.sum(dot32(perm, hid[...]), 1, keepdims=True)
    hidden_share = dot32(perm, hid[:, share_of(tp)])

    pltpu.make_async_copy(weights, weights, load_sem.at[1]).wait()
    received(spread.at[pl.ds(1, n_ep - 1)], h_recv.at[0])
    lhs = spread[...].reshape(n_ep * rows, depth)

    quad = GROUP_SIZE
    far_quads = range(1, n_ep // quad)
    bounds = [(0, cols), (cols, 2 * cols + DH), (2 * cols + DH, 3 * cols + DH), (3 * cols + DH, 4 * cols + DH)]
    cut = bounds[1][1]
    for i in range(4):
        part = dot32(lhs, weights[i])
        if i == 1:
            high, middle, low = three_parts(dot_t(lhs, gate_half))
            lane = lax.broadcasted_iota(jnp.int32, high.shape, 1)
            extra = jnp.where(lane < 2 * heads, high, jnp.where(lane < 4 * heads, middle, low))
            part = jnp.concatenate([part, extra], 1)
        span = slice(*bounds[i])
        proj_send[:, :, span] = part.astype(jnp.bfloat16).reshape(n_ep, rows, part.shape[1])
        proj_own[:, span] = part[:rows]
        for f in far_quads:
            far_own[f - 1, :, span] = part[f * quad * rows : (f * quad + 1) * rows]
        for f in far_quads:
            for j in range(quad - 1, 0, -1):
                remote(
                    proj_send.at[f * quad + j, :, span],
                    far_recv.at[f - 1, j - 1, :, span],
                    f_send.at[0],
                    f_recv.at[i],
                    (ep_peer[j], tp),
                ).start()
    for i in range(4):
        span = slice(*bounds[i])
        for j in range(quad - 1, 0, -1):
            remote(
                proj_send.at[j, :, span], proj_recv.at[j, :, span], p_send.at[0], p_recv.at[i], (ep_peer[j], tp)
            ).start()
    for i in range(4):
        span = slice(*bounds[i])
        received(far_recv.at[:, :, :, span], f_recv.at[i])
        for f in far_quads:
            summed = far_own[f - 1, :, span]
            for j in range(1, quad):
                summed += far_recv[f - 1, j - 1, :, span].astype(jnp.float32)
            if i < 2:
                source, target = cross_send.at[f - 1, :, span], cross_recv.at[f - 1, :, span]
                cross_send[f - 1, :, span] = summed
            else:
                span2 = slice(span.start - cut, span.stop - cut)
                source, target = cross_send2.at[f - 1, :, span2], cross_recv2.at[f - 1, :, span2]
                cross_send2[f - 1, :, span2] = summed.astype(jnp.bfloat16)
            remote(source, target, c_send.at[i // 2], c_recv.at[i], (ep_peer[f * quad], tp)).start()

    down_load.wait()
    gate_load.wait()
    up_load.wait()
    for j in range(n_y):
        place = share_of(2 * y_from[j] + 1 - core)
        remote(wg_buf.at[place], wg_other.at[j], w_send.at[0], w_recv.at[0], partner).start()
        remote(wu_buf.at[place], wu_other.at[j], w_send.at[1], w_recv.at[1], partner).start()
        theirs = wd_buf.at[:, share_of(2 * y_peer[j] + 1 - core)]
        remote(theirs, wd_other.at[j], w_send.at[2], w_recv.at[2], partner).start()

    def total(i):
        span = slice(*bounds[i])
        result = proj_own[:, span]
        received(proj_recv.at[pl.ds(1, quad - 1), :, span], p_recv.at[i])
        if i < 2:
            received(cross_recv.at[:, :, span], c_recv.at[i])
        else:
            received(cross_recv2.at[:, :, slice(span.start - cut, span.stop - cut)], c_recv.at[i])
        for j in range(1, quad):
            result += proj_recv[j, :, span].astype(jnp.float32)
        for f in far_quads:
            if i < 2:
                result += cross_recv[f - 1, :, span]
            else:
                result += cross_recv2[f - 1, :, span.start - cut : span.stop - cut].astype(jnp.float32)
        return result

    queries = total(0)
    read_old = []
    for h in range(heads):
        query = queries[:, h * DH : (h + 1) * DH]
        high = query.astype(jnp.bfloat16).astype(jnp.float32)
        both = jnp.concatenate([high, query - high], 0)
        row_of = lax.rem(lax.broadcasted_iota(jnp.int32, both.shape, 0), rows)
        spread_query = [jnp.where(row_of == b, both, 0.0).astype(jnp.bfloat16) for b in range(rows)]
        read = dot32(jnp.concatenate(spread_query, 1), mem_half[h])
        read_old.append(read[:rows] + read[rows:])
    second_total = total(1)
    keys = second_total[:, :cols] * DH ** (-0.5)
    gates = second_total[:, cols:]
    gates = gates + pltpu.roll(gates, DH - 2 * heads, 1) + pltpu.roll(gates, DH - 4 * heads, 1)
    scores = []
    for h in range(heads):
        span = slice(h * DH, (h + 1) * DH)
        scores.append(jnp.sum(queries[:, span] * keys[:, span], 1, keepdims=True))
    values = total(2)
    value_buf[...] = values
    last = total(3)
    mixed = []
    for h in range(heads):
        span = slice(h * DH, (h + 1) * DH)
        log_input = gates[:, h : h + 1] + input_bias[0:1, h : h + 1]
        forget = gates[:, heads + h : heads + h + 1] + forget_bias[0:1, h : h + 1]
        log_forget = jnp.minimum(forget, 0.0) - jnp.log1p(jnp.exp(-jnp.abs(forget)))
        carried = log_forget + to_column(max_state_t[h : h + 1, :])
        new_max = jnp.maximum(carried, log_input)
        keep = jnp.exp(carried - new_max)
        write = jnp.exp(log_input - new_max)
        max_out[h : h + 1, :] = to_row(new_max)
        keep_buf[h] = jnp.broadcast_to(keep, (rows, DH))
        write_keys[h * rows : (h + 1) * rows] = write * keys[:, span]
        readout = scores[h] * write * values[:, span] + keep * read_old[h]
        scaled = readout * lax.rsqrt(jnp.mean(readout * readout, -1, keepdims=True) + 1e-06)
        mixed.append((scaled * head_gain[:, span] * jax.nn.sigmoid(last[:, span])).astype(jnp.bfloat16))
    mixed_sorted = dot32(perm, jnp.concatenate(mixed, 1)).astype(jnp.bfloat16)

    out_load.wait()
    partial_sum = jnp.zeros((rows, 1), jnp.float32)
    order = list(range(n_tp - 1, -1, -1))
    for o in order:
        part = dot32(mixed_sorted, wo_buf[:, share_of(tp_peer[o])]).astype(jnp.bfloat16)
        mix_send[o] = part
        partial_sum += jnp.sum(part.astype(jnp.float32), 1, keepdims=True)
        if o:
            remote(mix_send.at[o], mix_recv.at[o], m_send.at[0], m_recv.at[0], (me, tp_peer[o])).start()
    high, middle, low = three_parts(partial_sum)
    lane = lax.broadcasted_iota(jnp.int32, (rows, DH), 1)
    parts = jnp.where(lane == 0, high, jnp.where(lane == 1, middle, jnp.where(lane == 2, low, 0.0)))
    sum_send[...] = parts.astype(jnp.bfloat16)
    others = pl.ds(1, n_tp - 1)
    for o in range(1, n_tp):
        remote(sum_send, sum_recv.at[o], u_send.at[0], u_recv.at[0], (me, tp_peer[o])).start()
    joined = res_alpha * hidden_share + mix_send[0].astype(jnp.float32)
    row_sum = res_alpha * hidden_sum + partial_sum
    received(mix_recv.at[others], m_recv.at[0])
    received(sum_recv.at[others], u_recv.at[0])
    for o in range(1, n_tp):
        joined += mix_recv[o].astype(jnp.float32)
        row_sum += jnp.sum(sum_recv[o].astype(jnp.float32), 1, keepdims=True)
    centred = joined - row_sum / width
    scaled_rows = centred * gain1[:, share_of(tp)]
    for g in range(groups):
        row_send[g] = scaled_rows[g * block : (g + 1) * block].astype(jnp.bfloat16)
    for k in far_first + [0]:
        for j in range(n_y - 1, -1, -1):
            if k or j:
                remote(
                    row_send.at[lax.div(ep_peer[k], GROUP_SIZE)],
                    arrived.at[j, k],
                    a_send.at[min(j, 1)],
                    a_recv.at[k],
                    (ep_peer[k], 2 * y_peer[j] + core),
                ).start()
    arrived[0, 0] = row_send[lax.div(me, GROUP_SIZE)]

    experts = expert_router_t.shape[0]
    expert_part = jnp.zeros((rows, experts), jnp.float32)
    group_part = jnp.zeros((rows, groups), jnp.float32)
    for piece in three_parts(scaled_rows):
        half = piece.astype(jnp.bfloat16)
        expert_part += dot_t(half, expert_router_t[:, share_of(tp)])
        group_part += dot_t(half, group_router_t[:, share_of(tp)])
    stat_send[...] = jnp.zeros_like(stat_send)
    stat_send[:, 0:experts] = expert_part
    stat_send[:, experts : experts + groups] = group_part
    stat_send[:, experts + groups : experts + groups + 1] = jnp.sum(centred * centred, 1, keepdims=True)
    for o in range(1, n_tp):
        remote(stat_send, stat_recv.at[o], s_send.at[0], s_recv.at[0], (me, tp_peer[o])).start()

    keys_t = write_keys[...].T
    for b in range(rows):
        for h in range(heads):
            old = mem_out[b, pl.ds(h, DH, stride=heads), :]
            column = keys_t[:, h * rows + b : h * rows + b + 1]
            value = value_buf[b : b + 1, h * DH : (h + 1) * DH]
            mem_out[b, pl.ds(h, DH, stride=heads), :] = keep_buf[h, b : b + 1, :] * old + column * value

    stat_total = stat_send[...]
    received(stat_recv.at[others], s_recv.at[0])
    for o in range(1, n_tp):
        stat_total += stat_recv[o]
    row_scale = lax.rsqrt(stat_total[:, experts + groups : experts + groups + 1] / width + 1e-05)
    logits = stat_total * row_scale
    lanes = lax.broadcasted_iota(jnp.int32, logits.shape, 1).astype(jnp.float32)
    pick = lambda index: jnp.sum(jnp.where(lanes == index, logits, 0.0), 1, keepdims=True)
    first_logit = pick(first)
    second_logit = pick(second)
    group_gate = jax.nn.sigmoid(pick(experts + jnp.floor(first / GROUP_SIZE)))
    weight1 = group_gate * jax.nn.sigmoid(first_logit - second_logit)
    weight2 = group_gate * jax.nn.sigmoid(second_logit - first_logit)
    mid = (scaled_rows * row_scale).astype(jnp.bfloat16).astype(jnp.float32)
    for g in range(groups):
        span = slice(g * block, (g + 1) * block)
        for slot, column in enumerate((first, second, weight1, weight2)):
            weight_buf[slot, g] = jnp.broadcast_to(column[span], (block, DH))
        mid_buf[g] = res_alpha * mid[span]

    received(wg_other, w_recv.at[0])
    received(wu_other, w_recv.at[1])
    received(wd_other, w_recv.at[2])
    for k in [0] + near_first:
        first_j = 0 if k else 1
        received(arrived.at[pl.ds(first_j, n_y - first_j), k], a_recv.at[k])
    count = n_ep * block
    hidden_units = wg_buf.shape[1]
    tokens32 = [arrived[j].astype(jnp.float32).reshape(count, share) for j in range(n_y)]
    tokens = [token.astype(jnp.bfloat16) for token in tokens32]
    places = [share_of(2 * y_from[j] + core) for j in range(n_y)]
    squares = jnp.zeros((count, DH), jnp.float32)
    for j in range(n_y):
        plain = tokens32[j] / gain1[:, places[j]]
        plain = plain * plain
        for c in range(share // DH):
            squares += plain[:, c * DH : (c + 1) * DH]
    square_send[...] = squares
    remote(square_send, square_recv, b_send.at[0], b_recv.at[0], partner).start()
    partial = []
    for side in range(2):
        gate_pre = jnp.zeros((count, hidden_units), jnp.float32)
        up_pre = jnp.zeros((count, hidden_units), jnp.float32)
        for j in range(n_y):
            gate_pre += dot32(tokens[j], wg_other[j] if side else wg_buf[places[j], :])
            up_pre += dot32(tokens[j], wu_other[j] if side else wu_buf[places[j], :])
        partial.append((gate_pre, up_pre))
        part_send[side, :, 0:hidden_units] = gate_pre.astype(jnp.bfloat16)
        part_send[side, :, hidden_units:] = up_pre.astype(jnp.bfloat16)
        remote(part_send.at[side], part_recv.at[side], d_send.at[0], d_recv.at[0], partner).start()
    received(square_recv, b_recv.at[0])
    squares += square_recv[...]
    token_scale = lax.rsqrt(jnp.sum(squares, 1, keepdims=True) / width + 1e-05)
    received(part_recv, d_recv.at[0])
    units = []
    for side in range(2):
        gate_pre = (partial[side][0] + part_recv[1 - side, :, 0:hidden_units].astype(jnp.float32)) * token_scale
        up_pre = (partial[side][1] + part_recv[1 - side, :, hidden_units:].astype(jnp.float32)) * token_scale
        units.append((gate_pre * jax.nn.sigmoid(gate_pre) * up_pre).astype(jnp.bfloat16))

    for j in range(n_y - 1, -1, -1):
        result = dot32(units[0], wd_buf[:, share_of(2 * y_peer[j] + core)]) + dot32(units[1], wd_other[j])
        for k in far_first + [0]:
            ret_send[j, k] = result[k * block : (k + 1) * block].astype(jnp.bfloat16)
        for k in far_first + [0]:
            if k or j:
                remote(
                    ret_send.at[j, k],
                    ret_recv.at[j, k],
                    r_send.at[min(j, 1)],
                    r_recv.at[k],
                    (ep_peer[k], 2 * y_peer[j] + core),
                ).start()
    for piece in range(groups):
        g = flip(lax.div(me, GROUP_SIZE), piece)
        gathered = mid_buf[g]
        for k in range(piece * GROUP_SIZE, (piece + 1) * GROUP_SIZE):
            expert = ep_peer[k].astype(jnp.float32)
            weight = jnp.where(weight_buf[0, g] == expert, weight_buf[2, g], 0.0)
            weight += jnp.where(weight_buf[1, g] == expert, weight_buf[3, g], 0.0)
            first_j = 0 if k else 1
            received(ret_recv.at[pl.ds(first_j, n_y - first_j), k], r_recv.at[k])
            result = jnp.zeros((block, share), jnp.float32)
            for j in range(n_y):
                result += (ret_recv[j, k] if k or j else ret_send[0, 0]).astype(jnp.float32)
            gathered += weight[:, 0:1] * result
        mid_buf[g] = gathered
    joined = mid_buf[...].reshape(rows, share)
    row_sum = jnp.sum(joined, -1, keepdims=True)
    square_sum = jnp.sum(joined * joined, -1, keepdims=True)
    stat2_send[...] = jnp.where(lane == 0, row_sum, square_sum)
    for o in range(1, n_tp):
        remote(stat2_send, stat2_recv.at[o], t_send.at[0], t_recv.at[0], (me, tp_peer[o])).start()
    received(stat2_recv.at[others], t_recv.at[0])
    for o in range(1, n_tp):
        row_sum += stat2_recv[o][:, 0:1]
        square_sum += stat2_recv[o][:, 1:2]
    row_mean = row_sum / width
    row_var = square_sum / width - row_mean * row_mean
    result = ((joined - row_mean) * lax.rsqrt(row_var + 1e-05) * gain2[...]).astype(jnp.bfloat16)
    out_ref[...] = dot32(perm_back, result).astype(jnp.bfloat16)
    rest = pl.ds(1, n_ep - 1)
    for ref, sem in (
        (spread.at[rest], h_send.at[0]),
        (far_recv, f_send.at[0]),
        (proj_recv.at[pl.ds(1, quad - 1)], p_send.at[0]),
        (cross_send, c_send.at[0]),
        (cross_send2, c_send.at[1]),
        (mix_send.at[others], m_send.at[0]),
        (sum_recv.at[others], u_send.at[0]),
        (arrived.at[0, rest], a_send.at[0]),
        (arrived.at[pl.ds(1, n_y - 1)], a_send.at[1]),
        (stat_recv.at[others], s_send.at[0]),
        (square_send, b_send.at[0]),
        (part_send, d_send.at[0]),
        (wg_other, w_send.at[0]),
        (wu_other, w_send.at[1]),
        (wd_other, w_send.at[2]),
        (ret_send.at[0, rest], r_send.at[0]),
        (ret_send.at[pl.ds(1, n_y - 1)], r_send.at[1]),
        (stat2_recv.at[others], t_send.at[0]),
    ):
        sent(ref, sem)


def layer(n_ep, n_tp, groups, *operands):
    hidden, wq, _, _, _, memory, w_out, w_gate, _, w_down = operands[:10]
    rows, width = hidden.shape
    heads = memory.shape[1] // DH
    depth, cols = wq.shape
    share = width // n_tp
    block = rows // groups
    n_y = n_tp // 2
    half, full = jnp.bfloat16, jnp.float32
    vmem = pl.BlockSpec(memory_space=pltpu.VMEM)
    anywhere = pl.BlockSpec(memory_space=pl.ANY)
    dma = pltpu.SemaphoreType.DMA
    count = n_ep * block
    wide = 4 * cols + DH
    n_far = n_ep // GROUP_SIZE - 1
    return pl.pallas_call(
        functools.partial(layer_kernel, n_ep, n_tp, groups),
        out_shape=(
            pltpu.VMEM((rows, share), half),
            pltpu.VMEM(memory.shape, full),
            pltpu.VMEM((heads, rows), full),
        ),
        in_specs=[anywhere] * len(operands),
        out_specs=(vmem, vmem, vmem),
        scratch_shapes=[pltpu.VMEM(x.shape, x.dtype) for x in operands[10:]]
        + [
            pltpu.VMEM((rows, width), half),
            pltpu.VMEM((4, depth, cols), half),
            pltpu.VMEM(w_out.shape, half),
            pltpu.VMEM(w_gate.shape[1:], half),
            pltpu.VMEM(w_gate.shape[1:], half),
            pltpu.VMEM(w_down.shape[1:], half),
            pltpu.VMEM((heads, rows * DH, DH), half),
            pltpu.VMEM((DH, depth), full),
            pltpu.VMEM((n_ep, rows, depth), half),
            pltpu.VMEM((n_ep, rows, wide), half),
            pltpu.VMEM((n_ep, rows, wide), half),
            pltpu.VMEM((rows, wide), full),
            pltpu.VMEM((n_far, rows, wide), full),
            pltpu.VMEM((n_far, GROUP_SIZE - 1, rows, wide), half),
            pltpu.VMEM((n_far, rows, 2 * cols + DH), full),
            pltpu.VMEM((n_far, rows, 2 * cols + DH), full),
            pltpu.VMEM((n_far, rows, 2 * cols), half),
            pltpu.VMEM((n_far, rows, 2 * cols), half),
            pltpu.VMEM((heads * rows, DH), full),
            pltpu.VMEM((heads, rows, DH), full),
            pltpu.VMEM((rows, cols), full),
            pltpu.VMEM((n_tp, rows, share), half),
            pltpu.VMEM((n_tp, rows, share), half),
            pltpu.VMEM((rows, DH), half),
            pltpu.VMEM((n_tp, rows, DH), half),
            pltpu.VMEM((groups, block, share), half),
            pltpu.VMEM((n_y, n_ep, block, share), half),
            pltpu.VMEM((count, DH), full),
            pltpu.VMEM((count, DH), full),
            pltpu.VMEM((rows, DH), full),
            pltpu.VMEM((n_tp, rows, DH), full),
            pltpu.VMEM((4, groups, block, DH), full),
            pltpu.VMEM((groups, block, share), full),
            pltpu.VMEM((2, count, 2 * w_gate.shape[2]), half),
            pltpu.VMEM((2, count, 2 * w_gate.shape[2]), half),
            pltpu.VMEM((n_y, share, w_gate.shape[2]), half),
            pltpu.VMEM((n_y, share, w_gate.shape[2]), half),
            pltpu.VMEM((n_y, w_down.shape[1], share), half),
            pltpu.VMEM((n_y, n_ep, block, share), half),
            pltpu.VMEM((n_y, n_ep, block, share), half),
            pltpu.VMEM((rows, DH), full),
            pltpu.VMEM((n_tp, rows, DH), full),
            dma((7,)),
            dma((1,)),
            dma((1,)),
            dma((1,)),
            dma((4,)),
            dma((1,)),
            dma((4,)),
            dma((2,)),
            dma((4,)),
            dma((1,)),
            dma((1,)),
            dma((1,)),
            dma((1,)),
            dma((2,)),
            dma((n_ep,)),
            dma((1,)),
            dma((1,)),
            dma((1,)),
            dma((1,)),
            dma((1,)),
            dma((1,)),
            dma((3,)),
            dma((3,)),
            dma((2,)),
            dma((n_ep,)),
            dma((1,)),
            dma((1,)),
        ],
        compiler_params=pltpu.CompilerParams(
            collective_id=0, has_side_effects=True, vmem_limit_bytes=VMEM_LIMIT
        ),
        name="layer",
    )(*operands)


def store_kernel(result, memory, new_max, out_ref, mem_out, max_out, sems):
    copies = [
        pltpu.make_async_copy(source, target, sems.at[i])
        for i, (source, target) in enumerate(((memory, mem_out), (result, out_ref), (new_max, max_out)))
    ]
    for copy in copies:
        copy.start()
    for copy in copies:
        copy.wait()


def store(*operands):
    anywhere = pl.BlockSpec(memory_space=pl.ANY)
    return pl.pallas_call(
        store_kernel,
        out_shape=tuple(jax.ShapeDtypeStruct(x.shape, x.dtype) for x in operands),
        in_specs=[anywhere] * 3,
        out_specs=(anywhere,) * 3,
        scratch_shapes=[pltpu.SemaphoreType.DMA((3,))],
        compiler_params=pltpu.CompilerParams(vmem_limit_bytes=1 << 20),
        name="store",
    )(*operands)


def kernel_body(
    hidden_in,
    w_query,
    w_key,
    w_value,
    w_outgate,
    w_igate,
    w_fgate,
    input_bias,
    forget_bias,
    mem_state,
    max_state,
    head_gain,
    w_output,
    first_gain,
    w_group_router,
    w_expert_router,
    expert_route,
    w_expgate,
    w_expup,
    w_expdown,
    second_gain,
):
    n_ep, n_tp = lax.axis_size("ep"), lax.axis_size("tp")
    rows, heads, flat = mem_state.shape
    groups = w_group_router.shape[1]
    memory = mem_state.reshape(rows, heads, DH, DH).transpose(0, 2, 1, 3).reshape(rows, DH * heads, DH)
    results = layer(
        n_ep,
        n_tp,
        groups,
        hidden_in,
        w_query,
        w_key,
        w_value,
        w_outgate,
        memory,
        w_output,
        w_expgate,
        w_expup,
        w_expdown,
        w_igate.T,
        w_fgate.T,
        input_bias[None],
        forget_bias[None],
        max_state.T,
        head_gain[None],
        first_gain[None],
        second_gain[None],
        w_group_router.T,
        w_expert_router.T,
        expert_route.T,
    )
    hidden_out, memory_next, max_next = store(*results)
    memory_next = memory_next.reshape(rows, DH, heads, DH).transpose(0, 2, 1, 3).reshape(rows, heads, flat)
    return (hidden_out, memory_next, max_next.T)


def either_body(*operands):
    hidden_in, w_query, group_router, experts = operands[0], operands[1], operands[14], operands[17]
    rows, width = hidden_in.shape
    n_ep, n_tp = lax.axis_size("ep"), lax.axis_size("tp")
    groups = group_router.shape[1]
    block, odd_rows = divmod(rows, groups)
    aligned = rows % 16 == 0 and block % 8 == 0 and odd_rows == 0 and experts.shape[0] == 1
    aligned = aligned and w_query.shape[0] % DH == 0 and width // n_tp % DH == 0
    aligned = aligned and n_tp % 2 == 0 and n_tp & (n_tp - 1) == 0 and n_ep & (n_ep - 1) == 0 and n_ep == groups * GROUP_SIZE and groups > 1
    return (kernel_body if aligned else body)(*operands)


def solution(mesh):
    return jax.shard_map(
        either_body,
        mesh=mesh,
        in_specs=(
            P("ep", None),
            P("ep", "tp"),
            P("ep", "tp"),
            P("ep", "tp"),
            P("ep", "tp"),
            P("ep", "tp"),
            P("ep", "tp"),
            P("tp"),
            P("tp"),
            P("ep", "tp", None),
            P("ep", "tp"),
            P("tp"),
            P("tp", None),
            P(),
            P(),
            P(),
            P("ep", None),
            P("ep", None, "tp"),
            P("ep", None, "tp"),
            P("ep", "tp", None),
            P("tp"),
        ),
        out_specs=(P("ep", "tp"), P("ep", "tp", None), P("ep", "tp")),
        check_vma=False,
    )
```
